32 devices in a mesh: grp: 2 (over y), ep: 4 (over z), tp: 4 (over x, core).
Axes of the slice: x: 2, y: 2, z: 4, core: 2. Of those that a mesh axis runs over, the one named last changes fastest.
Arguments:
- tokens: bfloat16 [512, 4096], P(('grp', 'ep'), 'tp'), parts along dimension 0, may hold values from -27 to 27
- group_choice: int32 [512], P(('grp', 'ep')), parts along dimension 0, may hold values from 0 to 1, as said below
- member_choice: int32 [512, 2], P(('grp', 'ep')), parts along dimension 0, may hold values from 0 to 1, as said below
- group_prob: float32 [512], P(('grp', 'ep')), parts along dimension 0, may hold values from 0.3 to 1
- member_score: float32 [512, 2], P(('grp', 'ep')), parts along dimension 0, may hold values from -4 to 4
- norm_gain: float32 [4096], P('tp'), may hold values from 0.1 to 1.9
- w_gate: bfloat16 [4, 4096, 1024], P('ep', 'tp'), may hold values from -0.09375 to 0.09375
- w_up: bfloat16 [4, 4096, 1024], P('ep', 'tp'), may hold values from -0.09375 to 0.09375
- w_down: bfloat16 [4, 1024, 4096], P('ep', None, 'tp'), may hold values from -0.1875 to 0.1875
- final_gain: float32 [4096], P('tp'), may hold values from 0.1 to 1.9
Outputs:
- mixed: bfloat16 [512, 4096], P(('grp', 'ep'), 'tp'), parts along dimension 0
The draws below stay inside these ranges and needn't reach their ends.
There are 2 independent parts, one for each index of `grp`. The reference program is written for one: setup_inputs(seed, part) draws one part's arguments, and reference() takes and returns one part's arrays. A program takes and returns all parts, laid end to end along the dimension named above; an argument that names none is the same for every part. Nothing has to cross between parts.
Inputs may be any that keep to these rules, and one draw needn't show every extreme that they name: `group_choice`: in each aligned block of 64 tokens every group is chosen by exactly 32 tokens. `member_choice`: each row names 2 different experts of its token's group. In each aligned block of 64 rows no expert (group and member together) is named by more than 32 rows, some expert is named by exactly 32 rows, and one expert is named by exactly 32 rows in every block.
All inputs are finite; a program needn't handle non-finite values.
Results may differ from the reference program's by a relative error of at most 0.017.
Values may be sent and summed in bfloat16 or wider, within the bound.
A program may use at most 64 MiB of HBM per device.

```python
import jax
import jax.numpy as jnp
from jax import lax

D = 4096
FF = 1024
TOK_DEV = 64
EXPERTS = 4
GROUPS = 2
PER_GROUP = 2
TOP = 2
CAP = 32
TOKENS = 256
N_EP = 4
N_TP = 4


def block_order(block_key):
    return jax.random.permutation(block_key, TOK_DEV)


def routing_draw(key):
    order_keys = jax.random.split(jax.random.fold_in(key, 101), N_EP)
    orderings = jax.vmap(block_order)(order_keys).astype(jnp.int32)
    groups_of = (orderings // CAP).astype(jnp.int32)
    favourite = jax.random.randint(jax.random.fold_in(key, 102), (GROUPS,), 0, PER_GROUP)
    coin_flip = jax.random.randint(jax.random.fold_in(key, 103), (N_EP, GROUPS), 0, 2)
    others = jax.random.randint(jax.random.fold_in(key, 104), (N_EP, GROUPS), 0, PER_GROUP)
    hot_member = jnp.where(coin_flip == 1, favourite[None, :], others)
    hot_member = hot_member.at[:, 0].set(favourite[0])
    token_hot = jnp.take_along_axis(hot_member, groups_of, axis=1)
    member_iota = jnp.arange(PER_GROUP, dtype=jnp.int32)
    raw_scores = jax.random.randint(jax.random.fold_in(key, 105), (N_EP, TOK_DEV, PER_GROUP), 0, 1 << 20)
    ranking = raw_scores * PER_GROUP + member_iota[None, None, :]
    ranking = jnp.where(member_iota[None, None, :] == token_hot[:, :, None], -1, ranking)
    members = jnp.argsort(ranking, axis=2)[:, :, :TOP]
    shuffle_scores = jax.random.randint(jax.random.fold_in(key, 106), (N_EP, TOK_DEV, TOP), 0, 1 << 20)
    shuffle_scores = shuffle_scores * TOP + jnp.arange(TOP, dtype=jnp.int32)[None, None, :]
    members = jnp.take_along_axis(members, jnp.argsort(shuffle_scores, axis=2), axis=2)
    return (groups_of.reshape(TOKENS).astype(jnp.int32), members.reshape(TOKENS, TOP).astype(jnp.int32))


def draw_group_choice(key, part):
    return routing_draw(key)[0]


def draw_member_choice(key, part):
    return routing_draw(key)[1]


def draw_tokens(key, part):
    col_pos = jnp.arange(D, dtype=jnp.float32) / D
    col_jitter = jax.random.uniform(jax.random.fold_in(key, 201), (D,), jnp.float32)
    col_scale = jnp.exp(jnp.log(10.0) * (0.5 * col_pos + 0.5 * col_jitter))
    row_scale = jnp.exp(jax.random.uniform(jax.random.fold_in(key, 202), (TOKENS, 1), jnp.float32, minval=jnp.log(0.3), maxval=jnp.log(3.0)))
    base = jnp.clip(jax.random.normal(jax.random.fold_in(key, 203), (TOKENS, D), jnp.float32), -6.0, 6.0)
    return (0.15 * base * row_scale * col_scale[None, :]).astype(jnp.bfloat16)


def block_scale(key, extent, cuts, low, top_value):
    gain, own = 1.0, jax.random.fold_in(key, 6)
    for dim, parts in cuts:
        heights = jnp.exp(jax.random.uniform(jax.random.fold_in(own, dim), (parts,), jnp.float32, low / len(cuts), top_value / len(cuts)))
        gain = gain * jnp.repeat(heights, extent[dim] // parts).reshape([-1 if axis == dim else 1 for axis in range(len(extent))])
    return gain


def normal_values(stream_key, extent, spread, reach, cuts=(), kind=jnp.bfloat16):
    values = jax.random.normal(stream_key, extent, jnp.float32) * spread
    if len(cuts) > 0:
        values = block_scale(stream_key, extent, cuts, -0.22, 0.18) * values
    return jnp.clip(values, min=-reach, max=reach).astype(kind)


def setup_inputs(seed: int = 0, part: int = 0) -> dict:
    streams_of = jax.random.split(jax.random.key(seed), 11)
    part_keys = jax.random.split(jax.random.fold_in(streams_of[10], part), 11)
    return {
        "tokens": draw_tokens(jax.random.fold_in(jax.random.fold_in(streams_of[10], part), 71), part),
        "group_choice": draw_group_choice(jax.random.fold_in(jax.random.fold_in(streams_of[10], part), 71), part),
        "member_choice": draw_member_choice(jax.random.fold_in(jax.random.fold_in(streams_of[10], part), 71), part),
        "group_prob": jnp.clip(0.3 + 0.7 * jax.random.uniform(part_keys[3], (TOKENS,), jnp.float32) ** block_scale(part_keys[3], (TOKENS,), ((0, 4),), -0.2, 0.2), 0.3, 1.0),
        "member_score": normal_values(part_keys[4], (TOKENS, TOP), 1.5, 4.0, ((0, 4),), jnp.float32),
        "norm_gain": jnp.clip(1.0 + 0.18 * jax.random.normal(streams_of[5], (D,), jnp.float32), 0.1, 1.9),
        "w_gate": normal_values(streams_of[6], (EXPERTS, D, FF), D ** -0.5, 0.09375, ((0, 4), (1, 4))),
        "w_up": normal_values(streams_of[7], (EXPERTS, D, FF), D ** -0.5, 0.09375, ((0, 4), (1, 4))),
        "w_down": normal_values(streams_of[8], (EXPERTS, FF, D), FF ** -0.5, 0.1875, ((0, 4), (2, 4))),
        "final_gain": jnp.clip(1.0 + 0.18 * jax.random.normal(streams_of[9], (D,), jnp.float32), 0.1, 1.9),
    }


EPS = 1e-06

def reference(tokens, group_choice, member_choice, group_prob, member_score, norm_gain, w_gate, w_up, w_down, final_gain):
    values = tokens.astype(jnp.float32)
    square_in = lax.optimization_barrier(jnp.sum(values * values, axis=1, keepdims=True))
    normed = (values * lax.rsqrt(square_in / D + EPS) * norm_gain.astype(jnp.float32)).astype(jnp.bfloat16)
    expert_ids = (group_choice[:, None] * PER_GROUP + member_choice).astype(jnp.int32)
    scores = jnp.exp(member_score)
    weights = group_prob[:, None] * scores / lax.optimization_barrier(jnp.sum(scores, axis=1, keepdims=True))
    blocks = normed.reshape(N_EP, TOK_DEV, D).astype(jnp.float32)
    slot_iota = jnp.arange(CAP, dtype=jnp.int32)

    def one_expert(carried, expert):
        chosen = expert_ids == expert
        counted = lax.optimization_barrier(jnp.sum(chosen.astype(jnp.int32), axis=1)).reshape(N_EP, TOK_DEV)
        weight_mine = lax.optimization_barrier(jnp.sum(jnp.where(chosen, weights, jnp.float32(0.0)), axis=1)).reshape(TOKENS, 1)
        position = jnp.cumsum(counted, axis=1) - counted
        slot_pick = ((position[:, None, :] == slot_iota[None, :, None]) & (counted[:, None, :] > 0)).astype(jnp.float32)
        rows_in = jnp.einsum('sct,std->scd', slot_pick, blocks).astype(jnp.bfloat16)
        rows_in = rows_in.reshape(N_EP * CAP, N_TP, D // N_TP).astype(jnp.float32)
        gate_w = lax.dynamic_index_in_dim(w_gate, expert, 0, keepdims=False).reshape(N_TP, D // N_TP, FF)
        up_w = lax.dynamic_index_in_dim(w_up, expert, 0, keepdims=False).reshape(N_TP, D // N_TP, FF)
        down_w = lax.dynamic_index_in_dim(w_down, expert, 0, keepdims=False)
        gate_part = jnp.einsum('rpd,pdf->prf', rows_in, gate_w.astype(jnp.float32)).astype(jnp.bfloat16)
        up_part = jnp.einsum('rpd,pdf->prf', rows_in, up_w.astype(jnp.float32)).astype(jnp.bfloat16)
        gate_part, up_part = lax.optimization_barrier((gate_part, up_part))
        gate_sum = lax.optimization_barrier(jnp.sum(gate_part.astype(jnp.float32), axis=0))
        up_sum = lax.optimization_barrier(jnp.sum(up_part.astype(jnp.float32), axis=0))
        hidden = (jax.nn.silu(gate_sum) * up_sum).astype(jnp.bfloat16)
        rows_out = jnp.dot(hidden, down_w, preferred_element_type=jnp.float32).astype(jnp.bfloat16)
        rows_out = rows_out.reshape(N_EP, CAP, D).astype(jnp.float32)
        returned = jnp.einsum('sct,scd->std', slot_pick, rows_out).reshape(TOKENS, D)
        return (carried + returned * weight_mine, expert)
    moe, unused = lax.scan(one_expert, jnp.zeros((TOKENS, D), jnp.float32), jnp.arange(EXPERTS, dtype=jnp.int32))
    summed = values + moe
    square_out = lax.optimization_barrier(jnp.sum(summed * summed, axis=1, keepdims=True))
    return (summed * lax.rsqrt(square_out / D + EPS) * final_gain.astype(jnp.float32)).astype(jnp.bfloat16)
```

```python
import functools

import jax
import jax.numpy as jnp
from jax import lax
from jax.experimental import pallas as pl
from jax.experimental.pallas import tpu as pltpu
from jax.sharding import PartitionSpec as P

EPS = 1e-06
MESH = pl.DeviceIdType.MESH
F32 = jnp.float32
BF16 = jnp.bfloat16
SEND = ((1, 2, 3), (3, 1, 2), (3, 1, 2), (1, 2, 3))
TAKE = ((1, 2, 3), (1, 3, 2), (3, 2, 1), (1, 3, 2))
BACK = (2, 3, 1)
AT_ONCE = 2
PLAN = (
    ("b", 0), ("a", 1), ("b", 1), ("a", 2), ("s", 0), ("b", 2), ("a", 3),
    ("c", 0), ("b", 3), ("s", 1), ("c", 1), ("s", 2), ("c", 2), ("s", 3), ("c", 3),
)
LANES = 128
CHUNKS = 4
VMEM_LIMIT = 56 * 2**20


def partner(me, s, n):
    out, bit = me, 1
    while bit < n:
        if s & bit:
            out = out + bit - 2 * bit * ((me // bit) % 2)
        bit *= 2
    return out


def parity(me, n):
    out, bit = 0, 1
    while bit < n:
        out = out + (me // bit) % 2
        bit *= 2
    return out % 2


def iota(shape, dim):
    return lax.broadcasted_iota(jnp.int32, shape, dim)


def to_row(col, width):
    n = col.shape[0]
    eye = iota((n, width), 0) == iota((n, width), 1)
    return jnp.sum(jnp.where(eye, col, 0.0), axis=0, keepdims=True)


def to_col(row, n):
    width = row.shape[1]
    eye = iota((n, width), 0) == iota((n, width), 1)
    return jnp.sum(jnp.where(eye, row, 0.0), axis=1, keepdims=True)


def pack(col):
    high = col.astype(BF16).astype(F32)
    middle = (col - high).astype(BF16).astype(F32)
    low = col - high - middle
    lane = iota((col.shape[0], LANES), 1)
    parts = jnp.where(lane == 0, high, jnp.where(lane == 1, middle, jnp.where(lane == 2, low, 0.0)))
    return parts.astype(BF16)


def unpack(parts):
    return jnp.sum(parts.astype(F32), axis=1, keepdims=True)


def kernel(
    cfg,
    x_hbm,
    group_hbm,
    member_hbm,
    prob_hbm,
    score_hbm,
    ngain_hbm,
    wg_hbm,
    wu_hbm,
    wd_hbm,
    out_ref,
    x_ref,
    group_ref,
    member_ref,
    prob_ref,
    score_ref,
    ngain_ref,
    wg,
    wu,
    wd,
    xs,
    xr,
    ps,
    pr,
    own,
    cs,
    cr,
    hs,
    hr,
    ob,
    ret,
    fs,
    fr,
    w_sem,
    send_sem,
    x_recv,
    p_recv,
    c_recv,
    h_recv,
    o_recv,
    f_recv,
):
    n_ep, n_tp, groups = cfg
    per_group = n_ep // groups
    tok, dim = x_ref.shape
    cap = tok // groups
    half = wg.shape[1] // 2
    full_width = dim * n_tp
    me_e = lax.axis_index("ep")
    me_t = lax.axis_index("tp")
    side = parity(me_t, n_tp)
    far = [s for s in range(1, n_tp) if parity(s, n_tp) == 0]
    each = n_ep // CHUNKS
    quarter = me_e // each

    def by_quarter(values):
        low, high = quarter % 2, quarter // 2
        return sum(
            v * (low if i % 2 else 1 - low) * (high if i // 2 else 1 - high) for i, v in enumerate(values)
        )

    def route(table, c, j):
        step = [0] * CHUNKS if c == 0 else [row[c - 1] for row in table]
        to = by_quarter([i ^ v for i, v in enumerate(step)]) * each + partner(me_e % each, j, each)
        return by_quarter(step) * each + j, to

    barrier = pltpu.get_barrier_semaphore()
    for s in range(1, n_ep):
        pl.semaphore_signal(barrier, inc=1, device_id={"ep": partner(me_e, s, n_ep)}, device_id_type=MESH)
    for s in range(1, n_tp):
        pl.semaphore_signal(barrier, inc=1, device_id={"tp": partner(me_t, s, n_tp)}, device_id_type=MESH)

    moves = (
        (group_hbm, group_ref),
        (x_hbm, x_ref),
        (ngain_hbm, ngain_ref),
        (wg_hbm.at[0], wg),
        (wu_hbm.at[0], wu),
        (member_hbm, member_ref),
        (prob_hbm, prob_ref),
        (score_hbm, score_ref),
        (wd_hbm.at[0], wd),
    )
    loads = [pltpu.make_async_copy(src, dst, w_sem.at[i]) for i, (src, dst) in enumerate(moves)]
    for load in loads:
        load.start()
    loads[0].wait()
    loads[1].wait()

    group_row = group_ref[...]
    rows8 = max(8, groups)
    onehot = (iota((rows8, tok), 0) == group_row).astype(F32)
    strict = (iota((tok, tok), 0) < iota((tok, tok), 1)).astype(F32)
    rank = jnp.dot(onehot.astype(BF16), strict.astype(BF16), preferred_element_type=F32)
    slot_row = jnp.sum(
        onehot * (iota((rows8, tok), 0).astype(F32) * cap + rank), axis=0, keepdims=True
    )
    picker = (iota((tok, tok), 0).astype(F32) == slot_row).astype(BF16)
    x = x_ref[...]
    xs[...] = jnp.dot(picker, x, preferred_element_type=F32).astype(BF16)

    def send(src, dst, sem, rsem, where):
        copy = pltpu.make_async_remote_copy(
            src_ref=src,
            dst_ref=dst,
            send_sem=send_sem.at[sem],
            recv_sem=rsem,
            device_id=where,
            device_id_type=MESH,
        )
        copy.start()

    def group_rows(e):
        return pl.ds(pl.multiple_of((e // per_group) * cap, cap), cap)

    def rows_of(first, count):
        return pl.ds(pl.multiple_of(first * cap, cap), count * cap)

    xr[pl.ds(0, cap), :] = xs[group_rows(me_e), :]

    def dispatch(c):
        for j in range(0 if c > 0 else 1, each):
            o, to = route(SEND, c, j)
            send(xs.at[group_rows(to)], xr.at[rows_of(o, 1)], 0, x_recv.at[o - 1], {"ep": to})

    def later():
        for c in range(AT_ONCE + 1, CHUNKS):
            dispatch(c)

    def enter():
        pl.semaphore_wait(barrier, n_ep - 1 + n_tp - 1)
        for c in range(AT_ONCE + 1):
            dispatch(c)
        if AT_ONCE + 1 < CHUNKS:
            pl.when(me_t % 2 == 0)(later)

    loads[2].wait()
    ngain = ngain_ref[...]
    squares = {}
    mate = {"tp": partner(me_t, 1, n_tp)}
    mine = pl.ds(pl.multiple_of(side * half, half), half)
    theirs = pl.ds(pl.multiple_of((1 - side) * half, half), half)
    body, tail = pl.ds(0, 2 * half), pl.ds(2 * half, LANES)

    def span(c):
        return rows_of(route(TAKE, c, 0)[0], each)

    def arrive(ref, sem):
        pltpu.make_async_copy(ref, ref, sem).wait()

    def stage_a(c):
        at = span(c)
        for j in range(0 if c > 0 else 1, each):
            o, _ = route(TAKE, c, j)
            arrive(xr.at[rows_of(o, 1)], x_recv.at[o - 1])
        vals = xr[at, :].astype(F32)
        squares[c] = jnp.sum(vals * vals, axis=1, keepdims=True)
        rows_in = (vals * ngain).astype(BF16)
        ps[at, pl.ds(0, half)] = jnp.dot(rows_in, wg[:, theirs], preferred_element_type=F32).astype(BF16)
        ps[at, pl.ds(half, half)] = jnp.dot(rows_in, wu[:, theirs], preferred_element_type=F32).astype(BF16)
        ps[at, tail] = pack(squares[c])
        if c > 0:
            send(ps.at[at], pr.at[at], 1, p_recv.at[c], mate)
        own[at, pl.ds(0, half)] = jnp.dot(rows_in, wg[:, mine], preferred_element_type=F32)
        own[at, pl.ds(half, half)] = jnp.dot(rows_in, wu[:, mine], preferred_element_type=F32)

    def stage_b(c):
        at = span(c)
        arrive(pr.at[at], p_recv.at[c])
        total = own[at, :] + pr[at, body].astype(F32)
        own[at, :] = total
        cs[at, body] = total.astype(BF16)
        squares[c] = squares[c] + unpack(pr[at, tail])
        cs[at, tail] = pack(squares[c])
        for i, s in enumerate(far):
            send(cs.at[at], cr.at[i, at], 2, c_recv.at[c, i], {"tp": partner(me_t, s, n_tp)})

    def stage_s(c):
        at = span(c)
        total, square = own[at, :], squares[c]
        for i in range(len(far)):
            arrive(cr.at[i, at], c_recv.at[c, i])
            total = total + cr[i, at, body].astype(F32)
            square = square + unpack(cr[i, at, tail])
        total = total * lax.rsqrt(square / full_width + EPS)
        g, u = total[:, :half], total[:, half:]
        hs[at, :] = (g / (1.0 + jnp.exp(-g)) * u).astype(BF16)
        send(hs.at[at], hr.at[at], 3, h_recv.at[c], mate)

    def stage_c(c):
        at = span(c)
        if c == 0:
            loads[8].wait()
        acc = jnp.dot(hs[at, :], wd[mine, :], preferred_element_type=F32)
        arrive(hr.at[at], h_recv.at[c])
        acc = acc + jnp.dot(hr[at, :], wd[theirs, :], preferred_element_type=F32)
        ob[at, :] = acc.astype(BF16)
        for j in range(0 if c > 0 else 1, each):
            o, to = route(TAKE, c, j)
            send(ob.at[rows_of(o, 1)], ret.at[rows_of(o, 1)], 4, o_recv.at[o - 1], {"ep": to})

    if each == 1:
        pl.when(quarter > 0)(enter)
    else:
        enter()
    loads[3].wait()
    loads[4].wait()
    stage_a(0)
    if each == 1:
        pl.when(quarter == 0)(enter)
    send(ps.at[span(0)], pr.at[span(0)], 1, p_recv.at[0], mate)
    for load in loads[5:8]:
        load.wait()
    scores = jnp.exp(score_ref[...])
    weights = prob_ref[...] * scores / jnp.sum(scores, axis=0, keepdims=True)
    slot_col = to_col(slot_row, tok).astype(jnp.int32)
    ids = group_row * per_group + member_ref[...]
    expert_cols = []
    for k in range(n_ep):
        named = jnp.where(ids == partner(me_e, k, n_ep), weights, 0.0)
        expert_cols.append(to_col(jnp.sum(named, axis=0, keepdims=True), tok))

    stages = {"a": stage_a, "b": stage_b, "s": stage_s, "c": stage_c}
    for stage, c in PLAN:
        stages[stage](c)
        if (stage, c) == ("a", 1) and AT_ONCE + 1 < CHUNKS:
            pl.when(me_t % 2 == 1)(later)

    summed = x.astype(F32)
    for k in [*range(each), *(q * each + j for q in BACK for j in range(each))]:
        e = partner(me_e, k, n_ep)
        block = pl.ds(k * cap, cap)
        if k > 0:
            arrive(ret.at[block], o_recv.at[k - 1])
            rows = ret[block, :]
        else:
            rows = ob[block, :]
        pick = (iota((tok, cap), 1) + (e // per_group) * cap == slot_col).astype(F32).astype(BF16)
        summed = summed + expert_cols[k] * jnp.dot(pick, rows, preferred_element_type=F32)

    square = jnp.sum(summed * summed, axis=1, keepdims=True)
    width = fs.shape[1]
    row = to_row(square, width)
    fs[...] = jnp.broadcast_to(row, (8, width))
    for s in range(1, n_tp):
        send(fs, fr.at[s - 1], 5, f_recv, {"tp": partner(me_t, s, n_tp)})

    arrive(fr, f_recv)
    for s in range(1, n_tp):
        row = row + fr[s - 1][0:1, :]
    out_ref[...] = summed * lax.rsqrt(to_col(row, tok) / full_width + EPS)

    others = pl.ds(cap, (n_ep - 1) * cap)
    for i, ref in enumerate((xr.at[others], pr, cr, hr, ret.at[others], fr)):
        arrive(ref, send_sem.at[i])


def solution(mesh):
    n_ep, n_tp = mesh.shape["ep"], mesh.shape["tp"]
    groups = max(2, n_ep // 8)
    n_far = n_tp // 2 - 1

    def local(tokens, group_choice, member_choice, group_prob, member_score, norm_gain, w_gate, w_up, w_down, final_gain):
        tok, dim = tokens.shape
        ff, top = w_gate.shape[2], member_choice.shape[1]
        cap = tok // groups
        all_rows = n_ep * cap
        out_width = -(-tok // 128) * 128
        vmem = pl.BlockSpec(memory_space=pltpu.VMEM)
        hbm = pl.BlockSpec(memory_space=pltpu.HBM)
        dma = pltpu.SemaphoreType.DMA
        normal = pl.pallas_call(
            functools.partial(kernel, (n_ep, n_tp, groups)),
            out_shape=pltpu.VMEM((tok, dim), F32),
            in_specs=[hbm] * 9,
            out_specs=vmem,
            scratch_shapes=[
                pltpu.VMEM((tok, dim), BF16),
                pltpu.VMEM((1, tok), jnp.int32),
                pltpu.VMEM((top, tok), jnp.int32),
                pltpu.VMEM((1, tok), F32),
                pltpu.VMEM((top, tok), F32),
                pltpu.VMEM((1, dim), F32),
                pltpu.VMEM((dim, ff), BF16),
                pltpu.VMEM((dim, ff), BF16),
                pltpu.VMEM((ff, dim), BF16),
                pltpu.VMEM((tok, dim), BF16),
                pltpu.VMEM((all_rows, dim), BF16),
                pltpu.VMEM((all_rows, ff + LANES), BF16),
                pltpu.VMEM((all_rows, ff + LANES), BF16),
                pltpu.VMEM((all_rows, ff), F32),
                pltpu.VMEM((all_rows, ff + LANES), BF16),
                pltpu.VMEM((n_far, all_rows, ff + LANES), BF16),
                pltpu.VMEM((all_rows, ff // 2), BF16),
                pltpu.VMEM((all_rows, ff // 2), BF16),
                pltpu.VMEM((all_rows, dim), BF16),
                pltpu.VMEM((all_rows, dim), BF16),
                pltpu.VMEM((8, out_width), F32),
                pltpu.VMEM((n_tp - 1, 8, out_width), F32),
                dma((9,)),
                dma((6,)),
                dma((n_ep - 1,)),
                dma((CHUNKS,)),
                dma((CHUNKS, n_far)),
                dma((CHUNKS,)),
                dma((n_ep - 1,)),
                dma,
            ],
            compiler_params=pltpu.CompilerParams(collective_id=0, has_side_effects=True, vmem_limit_bytes=VMEM_LIMIT),
        )(
            tokens,
            group_choice.reshape(1, tok),
            member_choice.T,
            group_prob.reshape(1, tok),
            member_score.T,
            norm_gain.reshape(1, dim),
            w_gate,
            w_up,
            w_down,
        )
        return (normal * final_gain[None, :]).astype(BF16)

    return jax.shard_map(
        local,
        mesh=mesh,
        in_specs=(
            P(("grp", "ep"), "tp"),
            P(("grp", "ep")),
            P(("grp", "ep"), None),
            P(("grp", "ep")),
            P(("grp", "ep"), None),
            P("tp"),
            P("ep", "tp", None),
            P("ep", "tp", None),
            P("ep", None, "tp"),
            P("tp"),
        ),
        out_specs=P(("grp", "ep"), "tp"),
        check_vma=False,
    )
```

```python
import functools

import jax
import jax.numpy as jnp
from jax import lax
from jax.experimental import pallas as pl
from jax.experimental.pallas import tpu as pltpu
from jax.sharding import PartitionSpec as P

EPS = 1e-06
MESH = pl.DeviceIdType.MESH
F32 = jnp.float32
BF16 = jnp.bfloat16
SEND = ((1, 2, 3), (3, 1, 2), (3, 1, 2), (1, 2, 3))
TAKE = ((1, 2, 3), (1, 3, 2), (3, 2, 1), (1, 3, 2))
BACK = (2, 3, 1)
AT_ONCE = 2
EVEN_PLAN = (
    ("b", 0), ("f", 0), ("a", 1), ("b", 1), ("a", 2), ("b", 2), ("s", 0), ("a", 3), ("c", 0), ("b", 3),
)
ODD_PLAN = (
    ("b", 0), ("f", 0), ("a", 1), ("a", 2), ("b", 1), ("a", 3), ("s", 0), ("b", 2), ("b", 3), ("c", 0),
)
PLAN = (
    ("s", 1), ("c", 1), ("s", 2), ("c", 2), ("s", 3), ("c", 3),
)
LANES = 128
CHUNKS = 4
PIECES = 2
FIRST = 2
RELAY_SEND = (2, 1)
RELAY_TAKE = ((2, 1, 3), (1, 2, 3), (2, 1, 3), (2, 3, 1))
VMEM_LIMIT = 56 * 2**20


def partner(me, s, n):
    out, bit = me, 1
    while bit < n:
        if s & bit:
            out = out + bit - 2 * bit * ((me // bit) % 2)
        bit *= 2
    return out


def parity(me, n):
    out, bit = 0, 1
    while bit < n:
        out = out + (me // bit) % 2
        bit *= 2
    return out % 2


def iota(shape, dim):
    return lax.broadcasted_iota(jnp.int32, shape, dim)


def to_row(col, width):
    n = col.shape[0]
    eye = iota((n, width), 0) == iota((n, width), 1)
    return jnp.sum(jnp.where(eye, col, 0.0), axis=0, keepdims=True)


def to_col(row, n):
    width = row.shape[1]
    eye = iota((n, width), 0) == iota((n, width), 1)
    return jnp.sum(jnp.where(eye, row, 0.0), axis=1, keepdims=True)


def pack(col):
    high = col.astype(BF16).astype(F32)
    middle = (col - high).astype(BF16).astype(F32)
    low = col - high - middle
    lane = iota((col.shape[0], LANES), 1)
    parts = jnp.where(lane == 0, high, jnp.where(lane == 1, middle, jnp.where(lane == 2, low, 0.0)))
    return parts.astype(BF16)


def unpack(parts):
    return jnp.sum(parts.astype(F32), axis=1, keepdims=True)


def kernel(
    cfg,
    x_hbm,
    group_hbm,
    member_hbm,
    prob_hbm,
    score_hbm,
    ngain_hbm,
    wg_hbm,
    wu_hbm,
    wd_hbm,
    out_ref,
    x_ref,
    group_ref,
    member_ref,
    prob_ref,
    score_ref,
    ngain_ref,
    wg,
    wu,
    wd,
    xs,
    xr,
    ps,
    pr,
    own,
    cs,
    cr,
    hs,
    hr,
    ob,
    ret,
    total_ref,
    split,
    fs,
    fr,
    w_sem,
    send_sem,
    x_recv,
    p_recv,
    c_recv,
    h_recv,
    o_recv,
    f_recv,
):
    n_ep, n_tp, groups = cfg
    per_group = n_ep // groups
    tok, dim = x_ref.shape
    cap = tok // groups
    half = wg.shape[1] // 2
    full_width = dim * n_tp
    me_e = lax.axis_index("ep")
    me_t = lax.axis_index("tp")
    side = parity(me_t, n_tp)
    far = [s for s in range(1, n_tp) if parity(s, n_tp) == 0]
    each = n_ep // CHUNKS
    relay = each == 1 and per_group == 2
    take = RELAY_TAKE if relay else TAKE
    met = [s for s in range(1, n_ep) if not relay or s < 3]
    quarter = me_e // each

    def by_quarter(values):
        low, high = quarter % 2, quarter // 2
        return sum(
            v * (low if i % 2 else 1 - low) * (high if i // 2 else 1 - high) for i, v in enumerate(values)
        )

    def route(table, c, j):
        step = [0] * CHUNKS if c == 0 else [row[c - 1] for row in table]
        to = by_quarter([i ^ v for i, v in enumerate(step)]) * each + partner(me_e % each, j, each)
        return by_quarter(step) * each + j, to

    barrier = pltpu.get_barrier_semaphore()
    for s in met:
        pl.semaphore_signal(barrier, inc=1, device_id={"ep": partner(me_e, s, n_ep)}, device_id_type=MESH)
    for s in range(1, n_tp):
        pl.semaphore_signal(barrier, inc=1, device_id={"tp": partner(me_t, s, n_tp)}, device_id_type=MESH)

    moves = (
        (group_hbm, group_ref),
        (x_hbm, x_ref),
        (ngain_hbm, ngain_ref),
        (wg_hbm.at[0], wg),
        (wu_hbm.at[0], wu),
        (member_hbm, member_ref),
        (prob_hbm, prob_ref),
        (score_hbm, score_ref),
        (wd_hbm.at[0], wd),
    )
    loads = [pltpu.make_async_copy(src, dst, w_sem.at[i]) for i, (src, dst) in enumerate(moves)]
    for load in loads:
        load.start()
    loads[0].wait()
    group_row = group_ref[...]
    rows8 = max(8, groups)
    onehot = (iota((rows8, tok), 0) == group_row).astype(F32)
    strict = (iota((tok, tok), 0) < iota((tok, tok), 1)).astype(F32)
    rank = jnp.dot(onehot.astype(BF16), strict.astype(BF16), preferred_element_type=F32)
    slot_row = jnp.sum(
        onehot * (iota((rows8, tok), 0).astype(F32) * cap + rank), axis=0, keepdims=True
    )
    picker = (iota((tok, tok), 0).astype(F32) == slot_row).astype(BF16)
    loads[1].wait()
    xs[...] = jnp.dot(picker, x_ref[...], preferred_element_type=F32).astype(BF16)

    def send(src, dst, sem, rsem, where):
        copy = pltpu.make_async_remote_copy(
            src_ref=src,
            dst_ref=dst,
            send_sem=send_sem.at[sem],
            recv_sem=rsem,
            device_id=where,
            device_id_type=MESH,
        )
        copy.start()

    def arrive(ref, sem):
        pltpu.make_async_copy(ref, ref, sem).wait()

    def group_rows(e):
        return pl.ds(pl.multiple_of((e // per_group) * cap, cap), cap)

    def rows_of(first, count):
        return pl.ds(pl.multiple_of(first * cap, cap), count * cap)

    xr[pl.ds(0, cap), :] = xs[group_rows(me_e), :]

    def dispatch(c):
        for j in range(0 if c > 0 else 1, each):
            o, to = route(SEND, c, j)
            send(xs.at[group_rows(to)], xr.at[rows_of(o, 1)], 0, x_recv.at[o - 1, 0], {"ep": to})

    def piece(ref, block, p):
        rows = cap // PIECES
        return ref.at[pl.ds(pl.multiple_of(block * cap + p * rows, rows), rows)]

    def stage_f(c):
        for p in range(PIECES):
            arrive(piece(xr, 2, p), x_recv.at[1, p])
            send(piece(xr, 2, p), piece(xr, 3, p), 0, x_recv.at[2, p], {"ep": partner(me_e, 1, n_ep)})

    def later():
        for c in range(AT_ONCE + 1, CHUNKS):
            dispatch(c)

    def enter():
        pl.semaphore_wait(barrier, len(met) + n_tp - 1)
        if relay:
            for o in RELAY_SEND:
                to = partner(me_e, o, n_ep)
                for p in range(PIECES):
                    send(piece(xs, to // per_group, p), piece(xr, o, p), 0, x_recv.at[o - 1, p], {"ep": to})
            return
        for c in range(AT_ONCE + 1):
            dispatch(c)
        if AT_ONCE + 1 < CHUNKS:
            pl.when(me_t % 2 == 0)(later)

    loads[2].wait()
    ngain = ngain_ref[...]
    mate = {"tp": partner(me_t, 1, n_tp)}
    mine = pl.ds(pl.multiple_of(side * half, half), half)
    theirs = pl.ds(pl.multiple_of((1 - side) * half, half), half)
    body, tail = pl.ds(0, 2 * half), pl.ds(2 * half, LANES)

    def span(c):
        return rows_of(route(take, c, 0)[0], each)

    def stage_a(c):
        at = span(c)
        if relay and c > 0:
            o, _ = route(take, c, 0)

            def landed():
                for p in range(PIECES):
                    arrive(piece(xr, o, p), x_recv.at[o - 1, p])

            pl.when(o != 2)(landed)
        for j in range(each if relay else 0 if c > 0 else 1, each):
            o, _ = route(take, c, j)
            arrive(xr.at[rows_of(o, 1)], x_recv.at[o - 1, 0])
        vals = xr[at, :].astype(F32)
        rows_in = (vals * ngain).astype(BF16)
        ps[at, pl.ds(0, half)] = jnp.dot(rows_in, wg[:, theirs], preferred_element_type=F32).astype(BF16)
        ps[at, pl.ds(half, half)] = jnp.dot(rows_in, wu[:, theirs], preferred_element_type=F32).astype(BF16)
        ps[at, tail] = pack(jnp.sum(vals * vals, axis=1, keepdims=True))
        if c > 0:
            send(ps.at[at], pr.at[at], 1, p_recv.at[c], mate)
        own[at, pl.ds(0, half)] = jnp.dot(rows_in, wg[:, mine], preferred_element_type=F32)
        own[at, pl.ds(half, half)] = jnp.dot(rows_in, wu[:, mine], preferred_element_type=F32)

    def stage_b(c):
        at = span(c)
        arrive(pr.at[at], p_recv.at[c])
        total = own[at, :] + pr[at, body].astype(F32)
        own[at, :] = total
        cs[at, body] = total.astype(BF16)
        cs[at, tail] = pack(unpack(ps[at, tail]) + unpack(pr[at, tail]))
        for i, s in enumerate(far):
            send(cs.at[at], cr.at[i, at], 2, c_recv.at[c, i], {"tp": partner(me_t, s, n_tp)})

    def stage_s(c):
        at = span(c)
        total, square = own[at, :], unpack(cs[at, tail])
        for i in range(len(far)):
            arrive(cr.at[i, at], c_recv.at[c, i])
            total = total + cr[i, at, body].astype(F32)
            square = square + unpack(cr[i, at, tail])
        total = total * lax.rsqrt(square / full_width + EPS)
        g, u = total[:, :half], total[:, half:]
        hs[at, :] = (g / (1.0 + jnp.exp(-g)) * u).astype(BF16)
        send(hs.at[at], hr.at[at], 3, h_recv.at[c], mate)

    def stage_c(c):
        at = span(c)
        if c == 0:
            loads[8].wait()
        acc = jnp.dot(hs[at, :], wd[mine, :], preferred_element_type=F32)
        arrive(hr.at[at], h_recv.at[c])
        acc = acc + jnp.dot(hr[at, :], wd[theirs, :], preferred_element_type=F32)
        ob[at, :] = acc.astype(BF16)
        for j in range(0 if c > 0 else 1, each):
            o, to = route(take, c, j)
            send(ob.at[rows_of(o, 1)], ret.at[rows_of(o, 1)], 4, o_recv.at[o - 1], {"ep": to})

    if each == 1:
        pl.when(me_e * n_tp + me_t >= FIRST)(enter)
    else:
        enter()
    loads[3].wait()
    loads[4].wait()
    stage_a(0)
    if each == 1:
        pl.when(me_e * n_tp + me_t < FIRST)(enter)
    send(ps.at[span(0)], pr.at[span(0)], 1, p_recv.at[0], mate)
    for load in loads[5:8]:
        load.wait()
    scores = jnp.exp(score_ref[...])
    weights = prob_ref[...] * scores / jnp.sum(scores, axis=0, keepdims=True)
    slots = slot_row.astype(jnp.int32)
    ids = group_row * per_group + member_ref[...]
    expert_cols = []
    for k in range(n_ep):
        e = partner(me_e, k, n_ep)
        named = jnp.sum(jnp.where(ids == e, weights, 0.0), axis=0, keepdims=True)
        here = iota((cap, tok), 0) + (e // per_group) * cap == slots
        expert_cols.append(jnp.sum(jnp.where(here, named, 0.0), axis=1, keepdims=True))
    slot_col = to_col(slot_row, tok).astype(jnp.int32)
    total_ref[...] = xs[...].astype(F32)

    stages = {"f": stage_f, "a": stage_a, "b": stage_b, "s": stage_s, "c": stage_c}
    def run(plan):
        for stage, c in plan:
            if relay or stage != "f":
                stages[stage](c)
            if (stage, c) == ("a", 1) and not relay and AT_ONCE + 1 < CHUNKS:
                pl.when(me_t % 2 == 1)(later)

    pl.when(me_t % 2 == 0)(functools.partial(run, EVEN_PLAN))
    pl.when(me_t % 2 == 1)(functools.partial(run, ODD_PLAN))
    run(PLAN)

    for k in [*range(each), *(q * each + j for q in BACK for j in range(each))]:
        block = pl.ds(k * cap, cap)
        if k > 0:
            arrive(ret.at[block], o_recv.at[k - 1])
        rows = (ret if k > 0 else ob)[block, :].astype(F32)
        at = group_rows(partner(me_e, k, n_ep))
        total_ref[at, :] = total_ref[at, :] + expert_cols[k] * rows

    summed = total_ref[...]
    square = jnp.sum(summed * summed, axis=1, keepdims=True)
    width = fs.shape[1]
    row = to_row(square, width)
    fs[...] = jnp.broadcast_to(row, (8, width))
    for s in range(1, n_tp):
        send(fs, fr.at[s - 1], 5, f_recv, {"tp": partner(me_t, s, n_tp)})

    high = summed.astype(BF16)
    rest = summed - high.astype(F32)
    middle = rest.astype(BF16)
    split[pl.ds(0, tok), :] = high
    split[pl.ds(tok, tok), :] = middle
    split[pl.ds(2 * tok, tok), :] = (rest - middle.astype(F32)).astype(BF16)
    lanes = iota((tok, 3 * tok), 1)
    back = jnp.where(lanes < tok, lanes, jnp.where(lanes < 2 * tok, lanes - tok, lanes - 2 * tok)) == slot_col
    out_ref[...] = jnp.dot(back.astype(F32).astype(BF16), split[...], preferred_element_type=F32)

    arrive(fr, f_recv)
    for s in range(1, n_tp):
        row = row + fr[s - 1][0:1, :]
    square = jnp.sum(jnp.where(iota((tok, width), 1) == slot_col, row, 0.0), axis=1, keepdims=True)
    out_ref[...] = out_ref[...] * lax.rsqrt(square / full_width + EPS)

    others = pl.ds(cap, (n_ep - 1) * cap)
    for i, ref in enumerate((xr.at[others], pr, cr, hr, ret.at[others], fr)):
        arrive(ref, send_sem.at[i])


def solution(mesh):
    n_ep, n_tp = mesh.shape["ep"], mesh.shape["tp"]
    groups = max(2, n_ep // 8)
    n_far = n_tp // 2 - 1

    def local(tokens, group_choice, member_choice, group_prob, member_score, norm_gain, w_gate, w_up, w_down, final_gain):
        tok, dim = tokens.shape
        ff, top = w_gate.shape[2], member_choice.shape[1]
        cap = tok // groups
        all_rows = n_ep * cap
        out_width = -(-tok // 128) * 128
        vmem = pl.BlockSpec(memory_space=pltpu.VMEM)
        hbm = pl.BlockSpec(memory_space=pltpu.HBM)
        dma = pltpu.SemaphoreType.DMA
        normal = pl.pallas_call(
            functools.partial(kernel, (n_ep, n_tp, groups)),
            out_shape=pltpu.VMEM((tok, dim), F32),
            in_specs=[hbm] * 9,
            out_specs=vmem,
            scratch_shapes=[
                pltpu.VMEM((tok, dim), BF16),
                pltpu.VMEM((1, tok), jnp.int32),
                pltpu.VMEM((top, tok), jnp.int32),
                pltpu.VMEM((1, tok), F32),
                pltpu.VMEM((top, tok), F32),
                pltpu.VMEM((1, dim), F32),
                pltpu.VMEM((dim, ff), BF16),
                pltpu.VMEM((dim, ff), BF16),
                pltpu.VMEM((ff, dim), BF16),
                pltpu.VMEM((tok, dim), BF16),
                pltpu.VMEM((all_rows, dim), BF16),
                pltpu.VMEM((all_rows, ff + LANES), BF16),
                pltpu.VMEM((all_rows, ff + LANES), BF16),
                pltpu.VMEM((all_rows, ff), F32),
                pltpu.VMEM((all_rows, ff + LANES), BF16),
                pltpu.VMEM((n_far, all_rows, ff + LANES), BF16),
                pltpu.VMEM((all_rows, ff // 2), BF16),
                pltpu.VMEM((all_rows, ff // 2), BF16),
                pltpu.VMEM((all_rows, dim), BF16),
                pltpu.VMEM((all_rows, dim), BF16),
                pltpu.VMEM((tok, dim), F32),
                pltpu.VMEM((3 * tok, dim), BF16),
                pltpu.VMEM((8, out_width), F32),
                pltpu.VMEM((n_tp - 1, 8, out_width), F32),
                dma((9,)),
                dma((6,)),
                dma((n_ep - 1, PIECES)),
                dma((CHUNKS,)),
                dma((CHUNKS, n_far)),
                dma((CHUNKS,)),
                dma((n_ep - 1,)),
                dma,
            ],
            compiler_params=pltpu.CompilerParams(collective_id=0, has_side_effects=True, vmem_limit_bytes=VMEM_LIMIT),
        )(
            tokens,
            group_choice.reshape(1, tok),
            member_choice.T,
            group_prob.reshape(1, tok),
            member_score.T,
            norm_gain.reshape(1, dim),
            w_gate,
            w_up,
            w_down,
        )
        return (normal * final_gain[None, :]).astype(BF16)

    return jax.shard_map(
        local,
        mesh=mesh,
        in_specs=(
            P(("grp", "ep"), "tp"),
            P(("grp", "ep")),
            P(("grp", "ep"), None),
            P(("grp", "ep")),
            P(("grp", "ep"), None),
            P("tp"),
            P("ep", "tp", None),
            P("ep", "tp", None),
            P("ep", None, "tp"),
            P("tp"),
        ),
        out_specs=P(("grp", "ep"), "tp"),
        check_vma=False,
    )
```

```python
import functools

import jax
import jax.numpy as jnp
from jax import lax
from jax.experimental import pallas as pl
from jax.experimental.pallas import tpu as pltpu
from jax.sharding import PartitionSpec as P

EPS = 1e-06
MESH = pl.DeviceIdType.MESH
F32 = jnp.float32
BF16 = jnp.bfloat16
SEND = ((1, 2, 3), (3, 1, 2), (3, 1, 2), (1, 2, 3))
TAKE = ((1, 2, 3), (1, 3, 2), (3, 2, 1), (1, 3, 2))
BACK = (2, 3, 1)
AT_ONCE = 2
EVEN_PLAN = (
    ("b", 0), ("w", 0), ("f", 0), ("a", 1), ("w", 1), ("b", 1), ("a", 2), ("w", 2), ("b", 2), ("s", 0), ("a", 3), ("w", 3), ("b", 3),
)
ODD_PLAN = (
    ("b", 0), ("f", 0), ("a", 1), ("a", 2), ("b", 1), ("a", 3), ("s", 0), ("b", 2), ("b", 3),
)
PLAN = (
    ("s", 1), ("c", 1), ("s", 2), ("c", 2), ("s", 3), ("c", 3), ("c", 0),
)
LANES = 128
CHUNKS = 4
PIECES = 2
FIRST = 2
W_PIECES = 8
W_CUTS = ((0, 2), (2, 4), (4, 6), (6, 8))
C_FIRST = 1
EARLY = 4
RELAY_SEND = (2, 1)
RELAY_TAKE = ((2, 1, 3), (1, 2, 3), (2, 1, 3), (2, 3, 1))
VMEM_LIMIT = 56 * 2**20


def partner(me, s, n):
    out, bit = me, 1
    while bit < n:
        if s & bit:
            out = out + bit - 2 * bit * ((me // bit) % 2)
        bit *= 2
    return out


def parity(me, n):
    out, bit = 0, 1
    while bit < n:
        out = out + (me // bit) % 2
        bit *= 2
    return out % 2


def iota(shape, dim):
    return lax.broadcasted_iota(jnp.int32, shape, dim)


def to_row(col, width):
    n = col.shape[0]
    eye = iota((n, width), 0) == iota((n, width), 1)
    return jnp.sum(jnp.where(eye, col, 0.0), axis=0, keepdims=True)


def to_col(row, n):
    width = row.shape[1]
    eye = iota((n, width), 0) == iota((n, width), 1)
    return jnp.sum(jnp.where(eye, row, 0.0), axis=1, keepdims=True)


def pack(col):
    high = col.astype(BF16).astype(F32)
    middle = (col - high).astype(BF16).astype(F32)
    low = col - high - middle
    lane = iota((col.shape[0], LANES), 1)
    parts = jnp.where(lane == 0, high, jnp.where(lane == 1, middle, jnp.where(lane == 2, low, 0.0)))
    return parts.astype(BF16)


def unpack(parts):
    return jnp.sum(parts.astype(F32), axis=1, keepdims=True)


def kernel(
    cfg,
    x_hbm,
    group_hbm,
    member_hbm,
    prob_hbm,
    score_hbm,
    ngain_hbm,
    wg_hbm,
    wu_hbm,
    wd_hbm,
    out_ref,
    x_ref,
    group_ref,
    member_ref,
    prob_ref,
    score_ref,
    ngain_ref,
    wg,
    wu,
    wds,
    xs,
    xr,
    ps,
    pr,
    own,
    cs,
    cr,
    hs,
    ob,
    ret,
    total_ref,
    split,
    fs,
    fr,
    w_sem,
    send_sem,
    x_recv,
    p_recv,
    c_recv,
    o_recv,
    f_recv,
    wd_recv,
):
    n_ep, n_tp, groups = cfg
    per_group = n_ep // groups
    tok, dim = x_ref.shape
    cap = tok // groups
    ff = wg.shape[1]
    full_width = dim * n_tp
    me_e = lax.axis_index("ep")
    me_t = lax.axis_index("tp")
    side = parity(me_t, n_tp)
    far = [s for s in range(1, n_tp) if parity(s, n_tp) == 0]
    each = n_ep // CHUNKS
    count = each * cap // 2
    units = max(1, each // 2)
    unit = count // units
    odd = me_t % 2
    relay = each == 1 and per_group == 2
    take = RELAY_TAKE if relay else TAKE
    met = [s for s in range(1, n_ep) if not relay or s < 3]
    quarter = me_e // each

    def by_quarter(values):
        low, high = quarter % 2, quarter // 2
        return sum(
            v * (low if i % 2 else 1 - low) * (high if i // 2 else 1 - high) for i, v in enumerate(values)
        )

    def route(table, c, j):
        step = [0] * CHUNKS if c == 0 else [row[c - 1] for row in table]
        to = by_quarter([i ^ v for i, v in enumerate(step)]) * each + partner(me_e % each, j, each)
        return by_quarter(step) * each + j, to

    barrier = pltpu.get_barrier_semaphore()
    for s in met:
        pl.semaphore_signal(barrier, inc=1, device_id={"ep": partner(me_e, s, n_ep)}, device_id_type=MESH)
    for s in range(1, n_tp):
        pl.semaphore_signal(barrier, inc=1, device_id={"tp": partner(me_t, s, n_tp)}, device_id_type=MESH)

    moves = (
        (group_hbm, group_ref),
        (x_hbm, x_ref),
        (ngain_hbm, ngain_ref),
        (wg_hbm.at[0], wg),
        (wu_hbm.at[0], wu),
        (member_hbm, member_ref),
        (prob_hbm, prob_ref),
        (score_hbm, score_ref),
        (wd_hbm.at[0], wds.at[odd]),
    )
    loads = [pltpu.make_async_copy(src, dst, w_sem.at[i]) for i, (src, dst) in enumerate(moves)]
    for load in loads:
        load.start()
    loads[0].wait()
    group_row = group_ref[...]
    rows8 = max(8, groups)
    onehot = (iota((rows8, tok), 0) == group_row).astype(F32)
    strict = (iota((tok, tok), 0) < iota((tok, tok), 1)).astype(F32)
    rank = jnp.dot(onehot.astype(BF16), strict.astype(BF16), preferred_element_type=F32)
    slot_row = jnp.sum(
        onehot * (iota((rows8, tok), 0).astype(F32) * cap + rank), axis=0, keepdims=True
    )
    picker = (iota((tok, tok), 0).astype(F32) == slot_row).astype(BF16)
    loads[1].wait()
    xs[...] = jnp.dot(picker, x_ref[...], preferred_element_type=F32).astype(BF16)

    def send(src, dst, sem, rsem, where):
        copy = pltpu.make_async_remote_copy(
            src_ref=src,
            dst_ref=dst,
            send_sem=send_sem.at[sem],
            recv_sem=rsem,
            device_id=where,
            device_id_type=MESH,
        )
        copy.start()

    def arrive(ref, sem):
        pltpu.make_async_copy(ref, ref, sem).wait()

    def group_rows(e):
        return pl.ds(pl.multiple_of((e // per_group) * cap, cap), cap)

    def rows_of(first, count):
        return pl.ds(pl.multiple_of(first * cap, cap), count * cap)

    xr[pl.ds(0, cap), :] = xs[group_rows(me_e), :]

    def dispatch(c):
        for j in range(0 if c > 0 else 1, each):
            o, to = route(SEND, c, j)
            send(xs.at[group_rows(to)], xr.at[rows_of(o, 1)], 0, x_recv.at[o - 1, 0], {"ep": to})

    def piece(ref, block, p):
        rows = cap // PIECES
        return ref.at[pl.ds(pl.multiple_of(block * cap + p * rows, rows), rows)]

    def stage_f(c):
        for p in range(PIECES):
            arrive(piece(xr, 2, p), x_recv.at[1, p])
            send(piece(xr, 2, p), piece(xr, 3, p), 0, x_recv.at[2, p], {"ep": partner(me_e, 1, n_ep)})

    def later():
        for c in range(AT_ONCE + 1, CHUNKS):
            dispatch(c)

    def greet():
        pl.semaphore_wait(barrier, len(met) + n_tp - 1)
        if relay:
            for o in RELAY_SEND:
                to = partner(me_e, o, n_ep)
                for p in range(PIECES):
                    send(piece(xs, to // per_group, p), piece(xr, o, p), 0, x_recv.at[o - 1, p], {"ep": to})
            return
        for c in range(AT_ONCE + 1):
            dispatch(c)
        if AT_ONCE + 1 < CHUNKS:
            pl.when(me_t % 2 == 0)(later)

    def enter():
        greet()
        if EARLY:
            pl.when(odd == 1)(push)

    def push():
        for c in range(EARLY):
            stage_w(c)

    loads[2].wait()
    ngain = ngain_ref[...]
    mate = {"tp": partner(me_t, 1, n_tp)}
    body, tail = pl.ds(0, 2 * ff), pl.ds(2 * ff, LANES)

    def mine(c):
        return pl.ds(c * count, count)

    def span(c):
        return rows_of(route(take, c, 0)[0], each)

    def stage_a(c):
        at = span(c)
        if relay and c > 0:
            o, _ = route(take, c, 0)

            def landed():
                for p in range(PIECES):
                    arrive(piece(xr, o, p), x_recv.at[o - 1, p])

            pl.when(o != 2)(landed)
        for j in range(each if relay else 0 if c > 0 else 1, each):
            o, _ = route(take, c, j)
            arrive(xr.at[rows_of(o, 1)], x_recv.at[o - 1, 0])
        vals = xr[at, :].astype(F32)
        rows_in = (vals * ngain).astype(BF16)
        square = jnp.sum(vals * vals, axis=1, keepdims=True)
        gate = jnp.dot(rows_in, wg[...], preferred_element_type=F32)
        up = jnp.dot(rows_in, wu[...], preferred_element_type=F32)

        def part(of, whose):
            return jnp.where(whose == 0, of[:count], of[count:])

        ps[mine(c), pl.ds(0, ff)] = part(gate, 1 - side).astype(BF16)
        ps[mine(c), pl.ds(ff, ff)] = part(up, 1 - side).astype(BF16)
        ps[mine(c), tail] = pack(part(square, 1 - side))
        if c > 0:
            send(ps.at[mine(c)], pr.at[mine(c)], 1, p_recv.at[c], mate)
        own[mine(c), pl.ds(0, ff)] = part(gate, side)
        own[mine(c), pl.ds(ff, ff)] = part(up, side)
        own[mine(c), tail] = jnp.broadcast_to(part(square, side), (count, LANES))

    def stage_b(c):
        at = mine(c)
        arrive(pr.at[at], p_recv.at[c])
        total = own[at, body] + pr[at, body].astype(F32)
        own[at, body] = total
        cs[at, body] = total.astype(BF16)
        square = own[at, tail] + unpack(pr[at, tail])
        own[at, tail] = square
        cs[at, tail] = pack(square[:, :1])
        for i, s in enumerate(far):
            send(cs.at[at], cr.at[i, at], 2, c_recv.at[c, i], {"tp": partner(me_t, s, n_tp)})

    def stage_s(c):
        at = mine(c)
        total, square = own[at, body], own[at, tail]
        for i in range(len(far)):
            arrive(cr.at[i, at], c_recv.at[c, i])
            total = total + cr[i, at, body].astype(F32)
            square = square + unpack(cr[i, at, tail])
        total = total * lax.rsqrt(square[:, :1] / full_width + EPS)
        g, u = total[:, :ff], total[:, ff:]
        hs[at, :] = (g / (1.0 + jnp.exp(-g)) * u).astype(BF16)

    def stage_w(c):
        piece_rows = ff // W_PIECES
        for p in range(*W_CUTS[c]):
            rows = pl.ds(p * piece_rows, piece_rows)
            send(wd_hbm.at[0, rows], wds.at[odd, rows], 3, wd_recv, mate)

    def stage_c(c):
        if c == C_FIRST:
            loads[8].wait()
            arrive(wds.at[1 - odd], wd_recv)
        hidden = hs[mine(c), :]
        for q in range(2):
            ob[q, mine(c), :] = jnp.dot(hidden, wds[q], preferred_element_type=F32).astype(BF16)
            for j in range(units):
                low, high = route(take, c, j), route(take, c, j + units if each > 1 else 0)
                o, to = (a + side * (b - a) for a, b in zip(low, high))
                block = o * (cap // unit) + (side if each == 1 else 0)
                src = ob.at[q, pl.ds(c * count + j * unit, unit)]
                dst = ret.at[pl.ds(pl.multiple_of(block * unit, unit), unit)]

                def stay():
                    dst[...] = src[...]

                def away():
                    send(src, dst, 4, o_recv.at[block], {"ep": to, "tp": me_t - odd + q})

                if c + j > 0:
                    away()
                else:
                    home = (odd == q) & (to == me_e)
                    pl.when(home)(stay)
                    pl.when(jnp.logical_not(home))(away)

    if each == 1:
        pl.when(me_e * n_tp + me_t >= FIRST)(enter)
    else:
        enter()
    loads[3].wait()
    loads[4].wait()
    stage_a(0)
    if each == 1:
        pl.when(me_e * n_tp + me_t < FIRST)(enter)
    send(ps.at[mine(0)], pr.at[mine(0)], 1, p_recv.at[0], mate)
    for load in loads[5:8]:
        load.wait()
    scores = jnp.exp(score_ref[...])
    weights = prob_ref[...] * scores / jnp.sum(scores, axis=0, keepdims=True)
    slots = slot_row.astype(jnp.int32)
    ids = group_row * per_group + member_ref[...]
    expert_cols = []
    for k in range(n_ep):
        e = partner(me_e, k, n_ep)
        named = jnp.sum(jnp.where(ids == e, weights, 0.0), axis=0, keepdims=True)
        here = iota((cap, tok), 0) + (e // per_group) * cap == slots
        expert_cols.append(jnp.sum(jnp.where(here, named, 0.0), axis=1, keepdims=True))
    slot_col = to_col(slot_row, tok).astype(jnp.int32)
    total_ref[...] = xs[...].astype(F32)

    stages = {"w": stage_w, "f": stage_f, "a": stage_a, "b": stage_b, "s": stage_s, "c": stage_c}
    def run(plan):
        for stage, c in plan:
            if relay or stage != "f":
                stages[stage](c)
            if (stage, c) == ("a", 1) and not relay and AT_ONCE + 1 < CHUNKS:
                pl.when(me_t % 2 == 1)(later)

    pl.when(me_t % 2 == 0)(functools.partial(run, EVEN_PLAN))
    pl.when(me_t % 2 == 1)(functools.partial(run, ODD_PLAN))
    run(PLAN)

    for k in [*range(each), *(q * each + j for q in BACK for j in range(each))]:
        block = pl.ds(k * cap, cap)
        if k > 0:
            for h in range(cap // unit):
                b = k * (cap // unit) + h
                arrive(ret.at[pl.ds(b * unit, unit)], o_recv.at[b])
        elif each == 1:
            b = 1 - side
            arrive(ret.at[pl.ds(pl.multiple_of(b * unit, unit), unit)], o_recv.at[b])
        else:
            pl.when(side == 1)(lambda: arrive(ret.at[pl.ds(0, unit)], o_recv.at[0]))
        rows = ret[block, :].astype(F32)
        at = group_rows(partner(me_e, k, n_ep))
        total_ref[at, :] = total_ref[at, :] + expert_cols[k] * rows

    summed = total_ref[...]
    square = jnp.sum(summed * summed, axis=1, keepdims=True)
    width = fs.shape[1]
    row = to_row(square, width)
    fs[...] = jnp.broadcast_to(row, (8, width))
    for s in range(1, n_tp):
        send(fs, fr.at[s - 1], 5, f_recv, {"tp": partner(me_t, s, n_tp)})

    high = summed.astype(BF16)
    rest = summed - high.astype(F32)
    middle = rest.astype(BF16)
    split[pl.ds(0, tok), :] = high
    split[pl.ds(tok, tok), :] = middle
    split[pl.ds(2 * tok, tok), :] = (rest - middle.astype(F32)).astype(BF16)
    lanes = iota((tok, 3 * tok), 1)
    back = jnp.where(lanes < tok, lanes, jnp.where(lanes < 2 * tok, lanes - tok, lanes - 2 * tok)) == slot_col
    out_ref[...] = jnp.dot(back.astype(F32).astype(BF16), split[...], preferred_element_type=F32)

    arrive(fr, f_recv)
    for s in range(1, n_tp):
        row = row + fr[s - 1][0:1, :]
    square = jnp.sum(jnp.where(iota((tok, width), 1) == slot_col, row, 0.0), axis=1, keepdims=True)
    out_ref[...] = out_ref[...] * lax.rsqrt(square / full_width + EPS)

    others = pl.ds(cap, (n_ep - 1) * cap)
    returns = pl.ds(unit, n_ep * cap - unit)
    for i, ref in enumerate((xr.at[others], pr, cr, wds.at[0], ret.at[returns], fr)):
        arrive(ref, send_sem.at[i])
    if each > 1:
        pl.when(side == 1)(lambda: arrive(ret.at[pl.ds(0, unit)], send_sem.at[4]))


def solution(mesh):
    n_ep, n_tp = mesh.shape["ep"], mesh.shape["tp"]
    groups = max(2, n_ep // 8)
    n_far = n_tp // 2 - 1

    def local(tokens, group_choice, member_choice, group_prob, member_score, norm_gain, w_gate, w_up, w_down, final_gain):
        tok, dim = tokens.shape
        ff, top = w_gate.shape[2], member_choice.shape[1]
        cap = tok // groups
        all_rows = n_ep * cap
        unit = min(cap, all_rows // CHUNKS // 2)
        out_width = -(-tok // 128) * 128
        vmem = pl.BlockSpec(memory_space=pltpu.VMEM)
        hbm = pl.BlockSpec(memory_space=pltpu.HBM)
        dma = pltpu.SemaphoreType.DMA
        normal = pl.pallas_call(
            functools.partial(kernel, (n_ep, n_tp, groups)),
            out_shape=pltpu.VMEM((tok, dim), F32),
            in_specs=[hbm] * 9,
            out_specs=vmem,
            scratch_shapes=[
                pltpu.VMEM((tok, dim), BF16),
                pltpu.VMEM((1, tok), jnp.int32),
                pltpu.VMEM((top, tok), jnp.int32),
                pltpu.VMEM((1, tok), F32),
                pltpu.VMEM((top, tok), F32),
                pltpu.VMEM((1, dim), F32),
                pltpu.VMEM((dim, ff), BF16),
                pltpu.VMEM((dim, ff), BF16),
                pltpu.VMEM((2, ff, dim), BF16),
                pltpu.VMEM((tok, dim), BF16),
                pltpu.VMEM((all_rows, dim), BF16),
                pltpu.VMEM((all_rows // 2, 2 * ff + LANES), BF16),
                pltpu.VMEM((all_rows // 2, 2 * ff + LANES), BF16),
                pltpu.VMEM((all_rows // 2, 2 * ff + LANES), F32),
                pltpu.VMEM((all_rows // 2, 2 * ff + LANES), BF16),
                pltpu.VMEM((n_far, all_rows // 2, 2 * ff + LANES), BF16),
                pltpu.VMEM((all_rows // 2, ff), BF16),
                pltpu.VMEM((2, all_rows // 2, dim), BF16),
                pltpu.VMEM((all_rows, dim), BF16),
                pltpu.VMEM((tok, dim), F32),
                pltpu.VMEM((3 * tok, dim), BF16),
                pltpu.VMEM((8, out_width), F32),
                pltpu.VMEM((n_tp - 1, 8, out_width), F32),
                dma((9,)),
                dma((6,)),
                dma((n_ep - 1, PIECES)),
                dma((CHUNKS,)),
                dma((CHUNKS, n_far)),
                dma((all_rows // unit,)),
                dma,
                dma,
            ],
            compiler_params=pltpu.CompilerParams(collective_id=0, has_side_effects=True, vmem_limit_bytes=VMEM_LIMIT),
        )(
            tokens,
            group_choice.reshape(1, tok),
            member_choice.T,
            group_prob.reshape(1, tok),
            member_score.T,
            norm_gain.reshape(1, dim),
            w_gate,
            w_up,
            w_down,
        )
        return (normal * final_gain[None, :]).astype(BF16)

    return jax.shard_map(
        local,
        mesh=mesh,
        in_specs=(
            P(("grp", "ep"), "tp"),
            P(("grp", "ep")),
            P(("grp", "ep"), None),
            P(("grp", "ep")),
            P(("grp", "ep"), None),
            P("tp"),
            P("ep", "tp", None),
            P("ep", "tp", None),
            P("ep", None, "tp"),
            P("tp"),
        ),
        out_specs=P(("grp", "ep"), "tp"),
        check_vma=False,
    )
```

```python
import functools

import jax
import jax.numpy as jnp
from jax import lax
from jax.experimental import pallas as pl
from jax.experimental.pallas import tpu as pltpu
from jax.sharding import PartitionSpec as P

EPS = 1e-06
MESH = pl.DeviceIdType.MESH
F32 = jnp.float32
BF16 = jnp.bfloat16
SEND = ((1, 2, 3), (3, 1, 2), (3, 1, 2), (1, 2, 3))
TAKE = ((1, 2, 3), (1, 3, 2), (3, 2, 1), (1, 3, 2))
BACK = (2, 3, 1)
AT_ONCE = 2
EVEN_PLAN = (
    ("b", 0), ("w", 0), ("f", 0), ("a", 1), ("w", 1), ("b", 1), ("a", 2), ("w", 2), ("b", 2), ("a", 3), ("w", 3), ("s", 0), ("b", 3),
)
ODD_PLAN = (
    ("w", 2), ("w", 3), ("b", 0), ("f", 0), ("a", 1), ("a", 2), ("b", 1), ("a", 3), ("s", 0), ("b", 2), ("b", 3),
)
PLAN = (
    ("s", 1), ("c", 1), ("s", 2), ("c", 2), ("s", 3), ("c", 3), ("c", 0),
)
LANES = 128
CHUNKS = 4
PIECES = 2
FIRST = 2
W_PIECES = 8
W_CUTS = ((0, 2), (2, 4), (4, 6), (6, 8))
C_FIRST = 1
EARLY = 2
SPLIT = (2,)
RELAY_SEND = (2, 1)
RELAY_TAKE = ((2, 1, 3), (1, 2, 3), (2, 1, 3), (2, 3, 1))
VMEM_LIMIT = 56 * 2**20


def partner(me, s, n):
    out, bit = me, 1
    while bit < n:
        if s & bit:
            out = out + bit - 2 * bit * ((me // bit) % 2)
        bit *= 2
    return out


def parity(me, n):
    out, bit = 0, 1
    while bit < n:
        out = out + (me // bit) % 2
        bit *= 2
    return out % 2


def iota(shape, dim):
    return lax.broadcasted_iota(jnp.int32, shape, dim)


def to_row(col, width):
    n = col.shape[0]
    eye = iota((n, width), 0) == iota((n, width), 1)
    return jnp.sum(jnp.where(eye, col, 0.0), axis=0, keepdims=True)


def to_col(row, n):
    width = row.shape[1]
    eye = iota((n, width), 0) == iota((n, width), 1)
    return jnp.sum(jnp.where(eye, row, 0.0), axis=1, keepdims=True)


def pack(col):
    high = col.astype(BF16).astype(F32)
    middle = (col - high).astype(BF16).astype(F32)
    low = col - high - middle
    lane = iota((col.shape[0], LANES), 1)
    parts = jnp.where(lane == 0, high, jnp.where(lane == 1, middle, jnp.where(lane == 2, low, 0.0)))
    return parts.astype(BF16)


def unpack(parts):
    return jnp.sum(parts.astype(F32), axis=1, keepdims=True)


def kernel(
    cfg,
    x_hbm,
    group_hbm,
    member_hbm,
    prob_hbm,
    score_hbm,
    ngain_hbm,
    wg_hbm,
    wu_hbm,
    wd_hbm,
    out_ref,
    x_ref,
    group_ref,
    member_ref,
    prob_ref,
    score_ref,
    ngain_ref,
    wg,
    wu,
    wds,
    xs,
    xr,
    ps,
    pr,
    own,
    cs,
    cr,
    hs,
    ob,
    ret,
    total_ref,
    split,
    fs,
    fr,
    w_sem,
    send_sem,
    x_recv,
    p_recv,
    c_recv,
    o_recv,
    f_recv,
    wd_recv,
):
    n_ep, n_tp, groups = cfg
    per_group = n_ep // groups
    tok, dim = x_ref.shape
    cap = tok // groups
    ff = wg.shape[1]
    full_width = dim * n_tp
    me_e = lax.axis_index("ep")
    me_t = lax.axis_index("tp")
    side = parity(me_t, n_tp)
    far = [s for s in range(1, n_tp) if parity(s, n_tp) == 0]
    each = n_ep // CHUNKS
    count = each * cap // 2
    units = max(1, each // 2)
    unit = count // units
    odd = me_t % 2
    relay = each == 1 and per_group == 2
    take = RELAY_TAKE if relay else TAKE
    met = [s for s in range(1, n_ep) if not relay or s < 3]
    quarter = me_e // each

    def by_quarter(values):
        low, high = quarter % 2, quarter // 2
        return sum(
            v * (low if i % 2 else 1 - low) * (high if i // 2 else 1 - high) for i, v in enumerate(values)
        )

    def route(table, c, j):
        step = [0] * CHUNKS if c == 0 else [row[c - 1] for row in table]
        to = by_quarter([i ^ v for i, v in enumerate(step)]) * each + partner(me_e % each, j, each)
        return by_quarter(step) * each + j, to

    barrier = pltpu.get_barrier_semaphore()
    for s in met:
        pl.semaphore_signal(barrier, inc=1, device_id={"ep": partner(me_e, s, n_ep)}, device_id_type=MESH)
    for s in range(1, n_tp):
        pl.semaphore_signal(barrier, inc=1, device_id={"tp": partner(me_t, s, n_tp)}, device_id_type=MESH)

    moves = (
        (group_hbm, group_ref),
        (x_hbm, x_ref),
        (ngain_hbm, ngain_ref),
        (wg_hbm.at[0], wg),
        (wu_hbm.at[0], wu),
        (member_hbm, member_ref),
        (prob_hbm, prob_ref),
        (score_hbm, score_ref),
        (wd_hbm.at[0], wds.at[odd]),
    )
    loads = [pltpu.make_async_copy(src, dst, w_sem.at[i]) for i, (src, dst) in enumerate(moves)]
    for load in loads:
        load.start()
    loads[0].wait()
    group_row = group_ref[...]
    rows8 = max(8, groups)
    onehot = (iota((rows8, tok), 0) == group_row).astype(F32)
    strict = (iota((tok, tok), 0) < iota((tok, tok), 1)).astype(F32)
    rank = jnp.dot(onehot.astype(BF16), strict.astype(BF16), preferred_element_type=F32)
    slot_row = jnp.sum(
        onehot * (iota((rows8, tok), 0).astype(F32) * cap + rank), axis=0, keepdims=True
    )
    picker = (iota((tok, tok), 0).astype(F32) == slot_row).astype(BF16)
    loads[1].wait()
    xs[...] = jnp.dot(picker, x_ref[...], preferred_element_type=F32).astype(BF16)

    def send(src, dst, sem, rsem, where):
        copy = pltpu.make_async_remote_copy(
            src_ref=src,
            dst_ref=dst,
            send_sem=send_sem.at[sem],
            recv_sem=rsem,
            device_id=where,
            device_id_type=MESH,
        )
        copy.start()

    def arrive(ref, sem):
        pltpu.make_async_copy(ref, ref, sem).wait()

    def group_rows(e):
        return pl.ds(pl.multiple_of((e // per_group) * cap, cap), cap)

    def rows_of(first, count):
        return pl.ds(pl.multiple_of(first * cap, cap), count * cap)

    xr[pl.ds(0, cap), :] = xs[group_rows(me_e), :]

    def dispatch(c):
        for j in range(0 if c > 0 else 1, each):
            o, to = route(SEND, c, j)
            send(xs.at[group_rows(to)], xr.at[rows_of(o, 1)], 0, x_recv.at[o - 1, 0], {"ep": to})

    def piece(ref, block, p):
        rows = cap // PIECES
        return ref.at[pl.ds(pl.multiple_of(block * cap + p * rows, rows), rows)]

    def stage_f(c):
        for p in range(PIECES):
            arrive(piece(xr, 2, p), x_recv.at[1, p])
            send(piece(xr, 2, p), piece(xr, 3, p), 0, x_recv.at[2, p], {"ep": partner(me_e, 1, n_ep)})

    def later():
        for c in range(AT_ONCE + 1, CHUNKS):
            dispatch(c)

    def greet():
        pl.semaphore_wait(barrier, len(met) + n_tp - 1)
        if relay:
            for o in RELAY_SEND:
                to = partner(me_e, o, n_ep)
                for p in range(PIECES):
                    send(piece(xs, to // per_group, p), piece(xr, o, p), 0, x_recv.at[o - 1, p], {"ep": to})
            return
        for c in range(AT_ONCE + 1):
            dispatch(c)
        if AT_ONCE + 1 < CHUNKS:
            pl.when(me_t % 2 == 0)(later)

    def enter():
        greet()
        if EARLY:
            pl.when(odd == 1)(push)

    def push():
        for c in range(EARLY):
            stage_w(c)

    loads[2].wait()
    ngain = ngain_ref[...]
    mate = {"tp": partner(me_t, 1, n_tp)}
    body, tail = pl.ds(0, 2 * ff), pl.ds(2 * ff, LANES)

    def mine(c):
        return pl.ds(c * count, count)

    def span(c):
        return rows_of(route(take, c, 0)[0], each)

    def stage_a(c):
        at = span(c)
        if relay and c > 0:
            o, _ = route(take, c, 0)

            def landed():
                for p in range(PIECES):
                    arrive(piece(xr, o, p), x_recv.at[o - 1, p])

            pl.when(o != 2)(landed)
        for j in range(each if relay else 0 if c > 0 else 1, each):
            o, _ = route(take, c, j)
            arrive(xr.at[rows_of(o, 1)], x_recv.at[o - 1, 0])
        here = mine(c)

        def products(rows):
            vals = xr[rows, :].astype(F32)
            rows_in = (vals * ngain).astype(BF16)
            square = jnp.sum(vals * vals, axis=1, keepdims=True)
            gate = jnp.dot(rows_in, wg[...], preferred_element_type=F32)
            return gate, jnp.dot(rows_in, wu[...], preferred_element_type=F32), square

        def hand_over(gate, up, square):
            ps[here, pl.ds(0, ff)] = gate.astype(BF16)
            ps[here, pl.ds(ff, ff)] = up.astype(BF16)
            ps[here, tail] = pack(square)
            if c > 0:
                send(ps.at[here], pr.at[here], 1, p_recv.at[c], mate)

        def keep(gate, up, square):
            own[here, pl.ds(0, ff)] = gate
            own[here, pl.ds(ff, ff)] = up
            own[here, tail] = jnp.broadcast_to(square, (count, LANES))

        if c in SPLIT:
            first = route(take, c, 0)[0] * cap
            for use, whose in ((hand_over, 1 - side), (keep, side)):
                use(*products(pl.ds(pl.multiple_of(first + whose * count, count), count)))
        else:
            both = products(at)
            for use, whose in ((hand_over, 1 - side), (keep, side)):
                use(*(jnp.where(whose == 0, of[:count], of[count:]) for of in both))

    def stage_b(c):
        at = mine(c)
        arrive(pr.at[at], p_recv.at[c])
        total = own[at, body] + pr[at, body].astype(F32)
        own[at, body] = total
        cs[at, body] = total.astype(BF16)
        square = own[at, tail] + unpack(pr[at, tail])
        own[at, tail] = square
        cs[at, tail] = pack(square[:, :1])
        for i, s in enumerate(far):
            send(cs.at[at], cr.at[i, at], 2, c_recv.at[c, i], {"tp": partner(me_t, s, n_tp)})

    def stage_s(c):
        at = mine(c)
        total, square = own[at, body], own[at, tail]
        for i in range(len(far)):
            arrive(cr.at[i, at], c_recv.at[c, i])
            total = total + cr[i, at, body].astype(F32)
            square = square + unpack(cr[i, at, tail])
        total = total * lax.rsqrt(square[:, :1] / full_width + EPS)
        g, u = total[:, :ff], total[:, ff:]
        hs[at, :] = (g / (1.0 + jnp.exp(-g)) * u).astype(BF16)

    def stage_w(c):
        piece_rows = ff // W_PIECES
        for p in range(*W_CUTS[c]):
            rows = pl.ds(p * piece_rows, piece_rows)
            send(wd_hbm.at[0, rows], wds.at[odd, rows], 3, wd_recv, mate)

    def stage_c(c):
        if c == C_FIRST:
            loads[8].wait()
            arrive(wds.at[1 - odd], wd_recv)
        hidden = hs[mine(c), :]
        for q in range(2):
            ob[q, mine(c), :] = jnp.dot(hidden, wds[q], preferred_element_type=F32).astype(BF16)
            for j in range(units):
                low, high = route(take, c, j), route(take, c, j + units if each > 1 else 0)
                o, to = (a + side * (b - a) for a, b in zip(low, high))
                block = o * (cap // unit) + (side if each == 1 else 0)
                src = ob.at[q, pl.ds(c * count + j * unit, unit)]
                dst = ret.at[pl.ds(pl.multiple_of(block * unit, unit), unit)]

                def stay():
                    dst[...] = src[...]

                def away():
                    send(src, dst, 4, o_recv.at[block], {"ep": to, "tp": me_t - odd + q})

                if c + j > 0:
                    away()
                else:
                    home = (odd == q) & (to == me_e)
                    pl.when(home)(stay)
                    pl.when(jnp.logical_not(home))(away)

    if each == 1:
        pl.when(me_e * n_tp + me_t >= FIRST)(enter)
    else:
        enter()
    loads[3].wait()
    loads[4].wait()
    stage_a(0)
    if each == 1:
        pl.when(me_e * n_tp + me_t < FIRST)(enter)
    send(ps.at[mine(0)], pr.at[mine(0)], 1, p_recv.at[0], mate)
    for load in loads[5:8]:
        load.wait()
    scores = jnp.exp(score_ref[...])
    weights = prob_ref[...] * scores / jnp.sum(scores, axis=0, keepdims=True)
    slots = slot_row.astype(jnp.int32)
    ids = group_row * per_group + member_ref[...]
    expert_cols = []
    for k in range(n_ep):
        e = partner(me_e, k, n_ep)
        named = jnp.sum(jnp.where(ids == e, weights, 0.0), axis=0, keepdims=True)
        here = iota((cap, tok), 0) + (e // per_group) * cap == slots
        expert_cols.append(jnp.sum(jnp.where(here, named, 0.0), axis=1, keepdims=True))
    slot_col = to_col(slot_row, tok).astype(jnp.int32)
    total_ref[...] = xs[...].astype(F32)

    stages = {"w": stage_w, "f": stage_f, "a": stage_a, "b": stage_b, "s": stage_s, "c": stage_c}
    def run(plan):
        for stage, c in plan:
            if relay or stage != "f":
                stages[stage](c)
            if (stage, c) == ("a", 1) and not relay and AT_ONCE + 1 < CHUNKS:
                pl.when(me_t % 2 == 1)(later)

    pl.when(me_t % 2 == 0)(functools.partial(run, EVEN_PLAN))
    pl.when(me_t % 2 == 1)(functools.partial(run, ODD_PLAN))
    run(PLAN)

    for k in [*range(each), *(q * each + j for q in BACK for j in range(each))]:
        block = pl.ds(k * cap, cap)
        if k > 0:
            for h in range(cap // unit):
                b = k * (cap // unit) + h
                arrive(ret.at[pl.ds(b * unit, unit)], o_recv.at[b])
        elif each == 1:
            b = 1 - side
            arrive(ret.at[pl.ds(pl.multiple_of(b * unit, unit), unit)], o_recv.at[b])
        else:
            pl.when(side == 1)(lambda: arrive(ret.at[pl.ds(0, unit)], o_recv.at[0]))
        rows = ret[block, :].astype(F32)
        at = group_rows(partner(me_e, k, n_ep))
        total_ref[at, :] = total_ref[at, :] + expert_cols[k] * rows

    summed = total_ref[...]
    square = jnp.sum(summed * summed, axis=1, keepdims=True)
    width = fs.shape[1]
    row = to_row(square, width)
    fs[...] = jnp.broadcast_to(row, (8, width))
    for s in range(1, n_tp):
        send(fs, fr.at[s - 1], 5, f_recv, {"tp": partner(me_t, s, n_tp)})

    high = summed.astype(BF16)
    rest = summed - high.astype(F32)
    middle = rest.astype(BF16)
    split[pl.ds(0, tok), :] = high
    split[pl.ds(tok, tok), :] = middle
    split[pl.ds(2 * tok, tok), :] = (rest - middle.astype(F32)).astype(BF16)
    lanes = iota((tok, 3 * tok), 1)
    back = jnp.where(lanes < tok, lanes, jnp.where(lanes < 2 * tok, lanes - tok, lanes - 2 * tok)) == slot_col
    out_ref[...] = jnp.dot(back.astype(F32).astype(BF16), split[...], preferred_element_type=F32)

    arrive(fr, f_recv)
    for s in range(1, n_tp):
        row = row + fr[s - 1][0:1, :]
    square = jnp.sum(jnp.where(iota((tok, width), 1) == slot_col, row, 0.0), axis=1, keepdims=True)
    out_ref[...] = out_ref[...] * lax.rsqrt(square / full_width + EPS)

    others = pl.ds(cap, (n_ep - 1) * cap)
    returns = pl.ds(unit, n_ep * cap - unit)
    for i, ref in enumerate((xr.at[others], pr, cr, wds.at[0], ret.at[returns], fr)):
        arrive(ref, send_sem.at[i])
    if each > 1:
        pl.when(side == 1)(lambda: arrive(ret.at[pl.ds(0, unit)], send_sem.at[4]))


def solution(mesh):
    n_ep, n_tp = mesh.shape["ep"], mesh.shape["tp"]
    groups = max(2, n_ep // 8)
    n_far = n_tp // 2 - 1

    def local(tokens, group_choice, member_choice, group_prob, member_score, norm_gain, w_gate, w_up, w_down, final_gain):
        tok, dim = tokens.shape
        ff, top = w_gate.shape[2], member_choice.shape[1]
        cap = tok // groups
        all_rows = n_ep * cap
        unit = min(cap, all_rows // CHUNKS // 2)
        out_width = -(-tok // 128) * 128
        vmem = pl.BlockSpec(memory_space=pltpu.VMEM)
        hbm = pl.BlockSpec(memory_space=pltpu.HBM)
        dma = pltpu.SemaphoreType.DMA
        normal = pl.pallas_call(
            functools.partial(kernel, (n_ep, n_tp, groups)),
            out_shape=pltpu.VMEM((tok, dim), F32),
            in_specs=[hbm] * 9,
            out_specs=vmem,
            scratch_shapes=[
                pltpu.VMEM((tok, dim), BF16),
                pltpu.VMEM((1, tok), jnp.int32),
                pltpu.VMEM((top, tok), jnp.int32),
                pltpu.VMEM((1, tok), F32),
                pltpu.VMEM((top, tok), F32),
                pltpu.VMEM((1, dim), F32),
                pltpu.VMEM((dim, ff), BF16),
                pltpu.VMEM((dim, ff), BF16),
                pltpu.VMEM((2, ff, dim), BF16),
                pltpu.VMEM((tok, dim), BF16),
                pltpu.VMEM((all_rows, dim), BF16),
                pltpu.VMEM((all_rows // 2, 2 * ff + LANES), BF16),
                pltpu.VMEM((all_rows // 2, 2 * ff + LANES), BF16),
                pltpu.VMEM((all_rows // 2, 2 * ff + LANES), F32),
                pltpu.VMEM((all_rows // 2, 2 * ff + LANES), BF16),
                pltpu.VMEM((n_far, all_rows // 2, 2 * ff + LANES), BF16),
                pltpu.VMEM((all_rows // 2, ff), BF16),
                pltpu.VMEM((2, all_rows // 2, dim), BF16),
                pltpu.VMEM((all_rows, dim), BF16),
                pltpu.VMEM((tok, dim), F32),
                pltpu.VMEM((3 * tok, dim), BF16),
                pltpu.VMEM((8, out_width), F32),
                pltpu.VMEM((n_tp - 1, 8, out_width), F32),
                dma((9,)),
                dma((6,)),
                dma((n_ep - 1, PIECES)),
                dma((CHUNKS,)),
                dma((CHUNKS, n_far)),
                dma((all_rows // unit,)),
                dma,
                dma,
            ],
            compiler_params=pltpu.CompilerParams(collective_id=0, has_side_effects=True, vmem_limit_bytes=VMEM_LIMIT),
        )(
            tokens,
            group_choice.reshape(1, tok),
            member_choice.T,
            group_prob.reshape(1, tok),
            member_score.T,
            norm_gain.reshape(1, dim),
            w_gate,
            w_up,
            w_down,
        )
        return (normal * final_gain[None, :]).astype(BF16)

    return jax.shard_map(
        local,
        mesh=mesh,
        in_specs=(
            P(("grp", "ep"), "tp"),
            P(("grp", "ep")),
            P(("grp", "ep"), None),
            P(("grp", "ep")),
            P(("grp", "ep"), None),
            P("tp"),
            P("ep", "tp", None),
            P("ep", "tp", None),
            P("ep", None, "tp"),
            P("tp"),
        ),
        out_specs=P(("grp", "ep"), "tp"),
        check_vma=False,
    )
```

```python
import functools

import jax
import jax.numpy as jnp
from jax import lax
from jax.experimental import pallas as pl
from jax.experimental.pallas import tpu as pltpu
from jax.sharding import PartitionSpec as P

EPS = 1e-06
MESH = pl.DeviceIdType.MESH
F32 = jnp.float32
BF16 = jnp.bfloat16
SEND = ((1, 2, 3), (3, 1, 2), (3, 1, 2), (1, 2, 3))
TAKE = ((1, 2, 3), (1, 3, 2), (3, 2, 1), (1, 3, 2))
BACK = (2, 3, 1)
AT_ONCE = 2
EVEN_PLAN = (
    ("b", 0), ("w", 0), ("f", 0), ("a", 1), ("w", 1), ("b", 1), ("a", 2), ("w", 2), ("b", 2), ("a", 3), ("w", 3), ("s", 0), ("b", 3),
)
ODD_PLAN = (
    ("w", 2), ("w", 3), ("b", 0), ("f", 0), ("a", 1), ("a", 2), ("b", 1), ("a", 3), ("s", 0), ("b", 2), ("b", 3),
)
PLAN = (
    ("s", 1), ("c", 1), ("s", 2), ("c", 2), ("s", 3), ("c", 3), ("c", 0),
)
LANES = 128
CHUNKS = 4
PIECES = 2
FIRST = 2
W_PIECES = 8
W_CUTS = ((0, 2), (2, 4), (4, 6), (6, 8))
C_FIRST = 1
EARLY = 2
SPLIT = (2,)
RELAY_SEND = (2, 1)
RELAY_TAKE = ((2, 1, 3), (1, 2, 3), (2, 1, 3), (2, 3, 1))
VMEM_LIMIT = 56 * 2**20


def partner(me, s, n):
    out, bit = me, 1
    while bit < n:
        if s & bit:
            out = out + bit - 2 * bit * ((me // bit) % 2)
        bit *= 2
    return out


def parity(me, n):
    out, bit = 0, 1
    while bit < n:
        out = out + (me // bit) % 2
        bit *= 2
    return out % 2


def iota(shape, dim):
    return lax.broadcasted_iota(jnp.int32, shape, dim)


def to_row(col, width):
    n = col.shape[0]
    eye = iota((n, width), 0) == iota((n, width), 1)
    return jnp.sum(jnp.where(eye, col, 0.0), axis=0, keepdims=True)


def to_col(row, n):
    width = row.shape[1]
    eye = iota((n, width), 0) == iota((n, width), 1)
    return jnp.sum(jnp.where(eye, row, 0.0), axis=1, keepdims=True)


def pack(col):
    high = col.astype(BF16).astype(F32)
    middle = (col - high).astype(BF16).astype(F32)
    low = col - high - middle
    lane = iota((col.shape[0], LANES), 1)
    parts = jnp.where(lane == 0, high, jnp.where(lane == 1, middle, jnp.where(lane == 2, low, 0.0)))
    return parts.astype(BF16)


def unpack(parts):
    return jnp.sum(parts.astype(F32), axis=1, keepdims=True)


def kernel(
    cfg,
    x_hbm,
    group_hbm,
    member_hbm,
    prob_hbm,
    score_hbm,
    ngain_hbm,
    wg_hbm,
    wu_hbm,
    wd_hbm,
    out_ref,
    x_ref,
    group_ref,
    member_ref,
    prob_ref,
    score_ref,
    ngain_ref,
    wg,
    wu,
    wds,
    xs,
    xr,
    ps,
    pr,
    own,
    cs,
    cr,
    hs,
    ob,
    ret,
    total_ref,
    split,
    fs,
    fr,
    w_sem,
    send_sem,
    x_recv,
    p_recv,
    c_recv,
    o_recv,
    f_recv,
    wd_recv,
):
    n_ep, n_tp, groups = cfg
    per_group = n_ep // groups
    tok, dim = x_ref.shape
    cap = tok // groups
    ff = wg.shape[1]
    full_width = dim * n_tp
    me_e = lax.axis_index("ep")
    me_t = lax.axis_index("tp")
    side = parity(me_t, n_tp)
    far = [s for s in range(1, n_tp) if parity(s, n_tp) == 0]
    each = n_ep // CHUNKS
    count = each * cap // 2
    units = max(1, each // 2)
    unit = count // units
    odd = me_t % 2
    relay = each == 1 and per_group == 2
    take = RELAY_TAKE if relay else TAKE
    met = [s for s in range(1, n_ep) if not relay or s < 3]
    quarter = me_e // each

    def by_quarter(values):
        low, high = quarter % 2, quarter // 2
        return sum(
            v * (low if i % 2 else 1 - low) * (high if i // 2 else 1 - high) for i, v in enumerate(values)
        )

    def route(table, c, j):
        step = [0] * CHUNKS if c == 0 else [row[c - 1] for row in table]
        to = by_quarter([i ^ v for i, v in enumerate(step)]) * each + partner(me_e % each, j, each)
        return by_quarter(step) * each + j, to

    barrier = pltpu.get_barrier_semaphore()
    for s in met:
        pl.semaphore_signal(barrier, inc=1, device_id={"ep": partner(me_e, s, n_ep)}, device_id_type=MESH)
    for s in range(1, n_tp):
        pl.semaphore_signal(barrier, inc=1, device_id={"tp": partner(me_t, s, n_tp)}, device_id_type=MESH)

    moves = (
        (group_hbm, group_ref),
        (x_hbm, x_ref),
        (ngain_hbm, ngain_ref),
        (wg_hbm.at[0], wg),
        (wu_hbm.at[0], wu),
        (member_hbm, member_ref),
        (prob_hbm, prob_ref),
        (score_hbm, score_ref),
        (wd_hbm.at[0], wds.at[odd]),
    )
    loads = [pltpu.make_async_copy(src, dst, w_sem.at[i]) for i, (src, dst) in enumerate(moves)]
    for load in loads:
        load.start()
    loads[0].wait()
    group_row = group_ref[...]
    rows8 = max(8, groups)
    onehot = (iota((rows8, tok), 0) == group_row).astype(F32)
    strict = (iota((tok, tok), 0) < iota((tok, tok), 1)).astype(F32)
    rank = jnp.dot(onehot.astype(BF16), strict.astype(BF16), preferred_element_type=F32)
    slot_row = jnp.sum(
        onehot * (iota((rows8, tok), 0).astype(F32) * cap + rank), axis=0, keepdims=True
    )
    picker = (iota((tok, tok), 0).astype(F32) == slot_row).astype(BF16)
    loads[1].wait()
    xs[...] = jnp.dot(picker, x_ref[...], preferred_element_type=F32).astype(BF16)

    def send(src, dst, sem, rsem, where):
        copy = pltpu.make_async_remote_copy(
            src_ref=src,
            dst_ref=dst,
            send_sem=send_sem.at[sem],
            recv_sem=rsem,
            device_id=where,
            device_id_type=MESH,
        )
        copy.start()

    def arrive(ref, sem):
        pltpu.make_async_copy(ref, ref, sem).wait()

    def group_rows(e):
        return pl.ds(pl.multiple_of((e // per_group) * cap, cap), cap)

    def rows_of(first, count):
        return pl.ds(pl.multiple_of(first * cap, cap), count * cap)

    xr[pl.ds(0, cap), :] = xs[group_rows(me_e), :]

    def dispatch(c):
        for j in range(0 if c > 0 else 1, each):
            o, to = route(SEND, c, j)
            send(xs.at[group_rows(to)], xr.at[rows_of(o, 1)], 0, x_recv.at[o - 1, 0], {"ep": to})

    def piece(ref, block, p):
        rows = cap // PIECES
        return ref.at[pl.ds(pl.multiple_of(block * cap + p * rows, rows), rows)]

    def stage_f(c):
        for p in range(PIECES):
            arrive(piece(xr, 2, p), x_recv.at[1, p])
            send(piece(xr, 2, p), piece(xr, 3, p), 0, x_recv.at[2, p], {"ep": partner(me_e, 1, n_ep)})

    def later():
        for c in range(AT_ONCE + 1, CHUNKS):
            dispatch(c)

    def greet():
        pl.semaphore_wait(barrier, len(met) + n_tp - 1)
        if relay:
            for o in RELAY_SEND:
                to = partner(me_e, o, n_ep)
                for p in range(PIECES):
                    send(piece(xs, to // per_group, p), piece(xr, o, p), 0, x_recv.at[o - 1, p], {"ep": to})
            return
        for c in range(AT_ONCE + 1):
            dispatch(c)
        if AT_ONCE + 1 < CHUNKS:
            pl.when(me_t % 2 == 0)(later)

    def enter():
        greet()
        if EARLY:
            pl.when(odd == 1)(push)

    def push():
        for c in range(EARLY):
            stage_w(c)

    loads[2].wait()
    ngain = ngain_ref[...]
    mate = {"tp": partner(me_t, 1, n_tp)}
    body, tail = pl.ds(0, 2 * ff), pl.ds(2 * ff, LANES)

    def mine(c):
        return pl.ds(c * count, count)

    def span(c):
        return rows_of(route(take, c, 0)[0], each)

    def stage_a(c):
        at = span(c)
        if relay and c > 0:
            o, _ = route(take, c, 0)

            def landed():
                for p in range(PIECES):
                    arrive(piece(xr, o, p), x_recv.at[o - 1, p])

            pl.when(o != 2)(landed)
        for j in range(each if relay else 0 if c > 0 else 1, each):
            o, _ = route(take, c, j)
            arrive(xr.at[rows_of(o, 1)], x_recv.at[o - 1, 0])
        here = mine(c)

        def products(rows):
            vals = xr[rows, :].astype(F32)
            rows_in = (vals * ngain).astype(BF16)
            square = jnp.sum(vals * vals, axis=1, keepdims=True)
            gate = jnp.dot(rows_in, wg[...], preferred_element_type=F32)
            return gate, jnp.dot(rows_in, wu[...], preferred_element_type=F32), square

        def hand_over(gate, up, square):
            ps[here, pl.ds(0, ff)] = gate.astype(BF16)
            ps[here, pl.ds(ff, ff)] = up.astype(BF16)
            ps[here, tail] = pack(square)
            if c > 0:
                send(ps.at[here], pr.at[here], 1, p_recv.at[c], mate)

        def keep(gate, up, square):
            own[here, pl.ds(0, ff)] = gate
            own[here, pl.ds(ff, ff)] = up
            own[here, tail] = jnp.broadcast_to(square, (count, LANES))

        if c in SPLIT:
            first = route(take, c, 0)[0] * cap
            for use, whose in ((hand_over, 1 - side), (keep, side)):
                use(*products(pl.ds(pl.multiple_of(first + whose * count, count), count)))
        else:
            both = products(at)
            for use, whose in ((hand_over, 1 - side), (keep, side)):
                use(*(jnp.where(whose == 0, of[:count], of[count:]) for of in both))

    def stage_b(c):
        at = mine(c)
        arrive(pr.at[at], p_recv.at[c])
        total = own[at, body] + pr[at, body].astype(F32)
        own[at, body] = total
        cs[at, body] = total.astype(BF16)
        square = own[at, tail] + unpack(pr[at, tail])
        own[at, tail] = square
        cs[at, tail] = pack(square[:, :1])
        for i, s in enumerate(far):
            send(cs.at[at], cr.at[i, at], 2, c_recv.at[c, i], {"tp": partner(me_t, s, n_tp)})

    def stage_s(c):
        at = mine(c)
        total, square = own[at, body], own[at, tail]
        for i in range(len(far)):
            arrive(cr.at[i, at], c_recv.at[c, i])
            total = total + cr[i, at, body].astype(F32)
            square = square + unpack(cr[i, at, tail])
        total = total * lax.rsqrt(square[:, :1] / full_width + EPS)
        g, u = total[:, :ff], total[:, ff:]
        hs[at, :] = (g / (1.0 + jnp.exp(-g)) * u).astype(BF16)

    def stage_w(c):
        piece_rows = ff // W_PIECES
        for p in range(*W_CUTS[c]):
            rows = pl.ds(p * piece_rows, piece_rows)
            send(wd_hbm.at[0, rows], wds.at[odd, rows], 3, wd_recv, mate)

    def stage_c(c):
        if c == C_FIRST:
            loads[8].wait()
            arrive(wds.at[1 - odd], wd_recv)
        hidden = hs[mine(c), :]
        for q in range(2):
            ob[q, mine(c), :] = jnp.dot(hidden, wds[q], preferred_element_type=F32).astype(BF16)
            for j in range(units):
                low, high = route(take, c, j), route(take, c, j + units if each > 1 else 0)
                o, to = (a + side * (b - a) for a, b in zip(low, high))
                block = o * (cap // unit) + (side if each == 1 else 0)
                src = ob.at[q, pl.ds(c * count + j * unit, unit)]
                dst = ret.at[pl.ds(pl.multiple_of(block * unit, unit), unit)]

                def stay():
                    dst[...] = src[...]

                def away():
                    send(src, dst, 4, o_recv.at[o], {"ep": to, "tp": me_t - odd + q})

                if c + j > 0:
                    away()
                else:
                    home = (odd == q) & (to == me_e)
                    pl.when(home)(stay)
                    pl.when(jnp.logical_not(home))(away)

    if each == 1:
        pl.when(me_e * n_tp + me_t >= FIRST)(enter)
    else:
        enter()
    loads[3].wait()
    loads[4].wait()
    stage_a(0)
    if each == 1:
        pl.when(me_e * n_tp + me_t < FIRST)(enter)
    send(ps.at[mine(0)], pr.at[mine(0)], 1, p_recv.at[0], mate)
    for load in loads[5:8]:
        load.wait()
    scores = jnp.exp(score_ref[...])
    weights = prob_ref[...] * scores / jnp.sum(scores, axis=0, keepdims=True)
    slots = slot_row.astype(jnp.int32)
    ids = group_row * per_group + member_ref[...]
    expert_cols = []
    for k in range(n_ep):
        e = partner(me_e, k, n_ep)
        named = jnp.sum(jnp.where(ids == e, weights, 0.0), axis=0, keepdims=True)
        here = iota((cap, tok), 0) + (e // per_group) * cap == slots
        expert_cols.append(jnp.sum(jnp.where(here, named, 0.0), axis=1, keepdims=True))
    slot_col = to_col(slot_row, tok).astype(jnp.int32)
    total_ref[...] = xs[...].astype(F32)

    stages = {"w": stage_w, "f": stage_f, "a": stage_a, "b": stage_b, "s": stage_s, "c": stage_c}
    def run(plan):
        for stage, c in plan:
            if relay or stage != "f":
                stages[stage](c)
            if (stage, c) == ("a", 1) and not relay and AT_ONCE + 1 < CHUNKS:
                pl.when(me_t % 2 == 1)(later)

    pl.when(me_t % 2 == 0)(functools.partial(run, EVEN_PLAN))
    pl.when(me_t % 2 == 1)(functools.partial(run, ODD_PLAN))
    run(PLAN)

    for k in [*range(each), *(q * each + j for q in BACK for j in range(each))]:
        block = pl.ds(k * cap, cap)
        if k > 0:
            arrive(ret.at[block], o_recv.at[k])
        elif each == 1:
            b = 1 - side
            arrive(ret.at[pl.ds(pl.multiple_of(b * unit, unit), unit)], o_recv.at[0])
        else:
            pl.when(side == 1)(lambda: arrive(ret.at[pl.ds(0, unit)], o_recv.at[0]))
        rows = ret[block, :].astype(F32)
        at = group_rows(partner(me_e, k, n_ep))
        total_ref[at, :] = total_ref[at, :] + expert_cols[k] * rows

    summed = total_ref[...]
    square = jnp.sum(summed * summed, axis=1, keepdims=True)
    width = fs.shape[1]
    row = to_row(square, width)
    fs[...] = jnp.broadcast_to(row, (8, width))
    for s in range(1, n_tp):
        send(fs, fr.at[s - 1], 5, f_recv, {"tp": partner(me_t, s, n_tp)})

    high = summed.astype(BF16)
    rest = summed - high.astype(F32)
    middle = rest.astype(BF16)
    split[pl.ds(0, tok), :] = high
    split[pl.ds(tok, tok), :] = middle
    split[pl.ds(2 * tok, tok), :] = (rest - middle.astype(F32)).astype(BF16)
    lanes = iota((tok, 3 * tok), 1)
    back = jnp.where(lanes < tok, lanes, jnp.where(lanes < 2 * tok, lanes - tok, lanes - 2 * tok)) == slot_col
    out_ref[...] = jnp.dot(back.astype(F32).astype(BF16), split[...], preferred_element_type=F32)

    arrive(fr, f_recv)
    for s in range(1, n_tp):
        row = row + fr[s - 1][0:1, :]
    square = jnp.sum(jnp.where(iota((tok, width), 1) == slot_col, row, 0.0), axis=1, keepdims=True)
    out_ref[...] = out_ref[...] * lax.rsqrt(square / full_width + EPS)

    others = pl.ds(cap, (n_ep - 1) * cap)
    returns = pl.ds(unit, n_ep * cap - unit)
    for i, ref in enumerate((xr.at[others], pr, cr, wds.at[0], ret.at[returns], fr)):
        arrive(ref, send_sem.at[i])
    if each > 1:
        pl.when(side == 1)(lambda: arrive(ret.at[pl.ds(0, unit)], send_sem.at[4]))


def solution(mesh):
    n_ep, n_tp = mesh.shape["ep"], mesh.shape["tp"]
    groups = max(2, n_ep // 8)
    n_far = n_tp // 2 - 1

    def local(tokens, group_choice, member_choice, group_prob, member_score, norm_gain, w_gate, w_up, w_down, final_gain):
        tok, dim = tokens.shape
        ff, top = w_gate.shape[2], member_choice.shape[1]
        cap = tok // groups
        all_rows = n_ep * cap
        out_width = -(-tok // 128) * 128
        vmem = pl.BlockSpec(memory_space=pltpu.VMEM)
        hbm = pl.BlockSpec(memory_space=pltpu.HBM)
        dma = pltpu.SemaphoreType.DMA
        normal = pl.pallas_call(
            functools.partial(kernel, (n_ep, n_tp, groups)),
            out_shape=pltpu.VMEM((tok, dim), F32),
            in_specs=[hbm] * 9,
            out_specs=vmem,
            scratch_shapes=[
                pltpu.VMEM((tok, dim), BF16),
                pltpu.VMEM((1, tok), jnp.int32),
                pltpu.VMEM((top, tok), jnp.int32),
                pltpu.VMEM((1, tok), F32),
                pltpu.VMEM((top, tok), F32),
                pltpu.VMEM((1, dim), F32),
                pltpu.VMEM((dim, ff), BF16),
                pltpu.VMEM((dim, ff), BF16),
                pltpu.VMEM((2, ff, dim), BF16),
                pltpu.VMEM((tok, dim), BF16),
                pltpu.VMEM((all_rows, dim), BF16),
                pltpu.VMEM((all_rows // 2, 2 * ff + LANES), BF16),
                pltpu.VMEM((all_rows // 2, 2 * ff + LANES), BF16),
                pltpu.VMEM((all_rows // 2, 2 * ff + LANES), F32),
                pltpu.VMEM((all_rows // 2, 2 * ff + LANES), BF16),
                pltpu.VMEM((n_far, all_rows // 2, 2 * ff + LANES), BF16),
                pltpu.VMEM((all_rows // 2, ff), BF16),
                pltpu.VMEM((2, all_rows // 2, dim), BF16),
                pltpu.VMEM((all_rows, dim), BF16),
                pltpu.VMEM((tok, dim), F32),
                pltpu.VMEM((3 * tok, dim), BF16),
                pltpu.VMEM((8, out_width), F32),
                pltpu.VMEM((n_tp - 1, 8, out_width), F32),
                dma((9,)),
                dma((6,)),
                dma((n_ep - 1, PIECES)),
                dma((CHUNKS,)),
                dma((CHUNKS, n_far)),
                dma((n_ep,)),
                dma,
                dma,
            ],
            compiler_params=pltpu.CompilerParams(collective_id=0, has_side_effects=True, vmem_limit_bytes=VMEM_LIMIT),
        )(
            tokens,
            group_choice.reshape(1, tok),
            member_choice.T,
            group_prob.reshape(1, tok),
            member_score.T,
            norm_gain.reshape(1, dim),
            w_gate,
            w_up,
            w_down,
        )
        return (normal * final_gain[None, :]).astype(BF16)

    return jax.shard_map(
        local,
        mesh=mesh,
        in_specs=(
            P(("grp", "ep"), "tp"),
            P(("grp", "ep")),
            P(("grp", "ep"), None),
            P(("grp", "ep")),
            P(("grp", "ep"), None),
            P("tp"),
            P("ep", "tp", None),
            P("ep", "tp", None),
            P("ep", None, "tp"),
            P("tp"),
        ),
        out_specs=P(("grp", "ep"), "tp"),
        check_vma=False,
    )
```
